32 devices in a mesh: sp: 8 (over z, y), tp: 4 (over x, core).
Axes of the slice: x: 2, y: 2, z: 4, core: 2. Of those that a mesh axis runs over, the one named last changes fastest.
Arguments:
- residual: bfloat16 [2048, 2048], P(('sp', 'tp')), may hold values from -6 to 6
- queries: bfloat16 [2048, 2048], P('sp', 'tp'), may hold values from -40 to 40
- key_rows: bfloat16 [2048, 1024], P('sp', 'tp'), may hold values from -40 to 40
- value_rows: bfloat16 [2048, 1024], P('sp', 'tp'), may hold values from -6 to 6
- forget_sums: float32 [2048, 16], P('sp', 'tp'), as said below
- out_weight: bfloat16 [2048, 2048], P('tp'), may hold values from -0.25 to 0.25
- norm_gain: float32 [2048], replicated, may hold values from 0.1 to 1.9
- expert_ids: int32 [2048, 4], P(('sp', 'tp')), may hold values from 0 to 7, all different within a row; in each aligned block of 64 rows (0 to 63, 64 to 127, ...) at most 64 rows name the same one
- route_weights: float32 [2048, 4], P(('sp', 'tp')), may hold values from 0.1 to 1
- expert_gate: bfloat16 [8, 2048, 384], P('sp'), may hold values from -0.125 to 0.125
- expert_up: bfloat16 [8, 2048, 384], P('sp'), may hold values from -0.125 to 0.125
- expert_down: bfloat16 [8, 384, 2048], P('sp'), may hold values from -0.3125 to 0.3125
- shared_gate: bfloat16 [2048, 384], replicated, may hold values from -0.125 to 0.125
- shared_up: bfloat16 [2048, 384], replicated, may hold values from -0.125 to 0.125
- shared_down: bfloat16 [384, 2048], replicated, may hold values from -0.3125 to 0.3125
Outputs:
- layer_out: bfloat16 [2048, 2048], P(('sp', 'tp'))
The draws below stay inside these ranges and needn't reach their ends.
Inputs may be any that keep to these rules, and one draw needn't show every extreme that they name: `forget_sums`: each head's column never rises from one position to the next. `expert_ids`: each row names 4 different experts; among the rows of one device no expert is named more than 64 times.
All inputs are finite; a program needn't handle non-finite values.
Results may differ from the reference program's by a relative error of at most 0.014.
Values may be sent and summed in bfloat16 or wider, within the bound.
A program may use at most 128 MiB of HBM per device.

```python
import math
import jax
import jax.numpy as jnp
import numpy as np
from jax import lax

D = 2048
HEADS = 16
KV_HEADS = 8
HEAD_DIM = 128
FE = 384
FS = 384
TOPK = 4
TOK_DEV = 256
EXPERTS = 8
TOKENS = 2048
ROWS = 64
CAP = 64


def query_key_pair(key):
    base_seed = jax.random.fold_in(key, 11)
    seed_list = jax.random.split(base_seed, 2)
    query_rows = 1.3 * jax.random.normal(seed_list[0], (TOKENS, HEADS * HEAD_DIM), jnp.float32)
    key_block = 1.3 * jax.random.normal(seed_list[1], (TOKENS, KV_HEADS * HEAD_DIM), jnp.float32)
    return (jnp.clip(query_rows, -40.0, 40.0), jnp.clip(key_block, -40.0, 40.0))


def draw_queries(key, part):
    return query_key_pair(key)[0].astype(jnp.bfloat16)


def draw_key_rows(key, part):
    return query_key_pair(key)[1].astype(jnp.bfloat16)


def draw_forget_sums(key, part):
    base_seed = jax.random.fold_in(key, 23)
    seed_list = jax.random.split(base_seed, 7)
    ordering = jax.random.permutation(seed_list[0], HEADS)
    slowly = ordering < HEADS // 2
    slow_rate = jax.random.uniform(seed_list[1], (HEADS,), jnp.float32, 0.25, 1.0) / TOKENS
    fast_rate = jnp.exp(jax.random.uniform(seed_list[2], (HEADS,), jnp.float32, math.log(0.01), math.log(1.0 / 30.0)))
    rates = jnp.where(slowly, slow_rate, fast_rate)
    block_count = TOKENS // TOK_DEV
    factor = jnp.exp(jax.random.uniform(seed_list[3], (block_count, 1), jnp.float32, -0.7, 0.7))
    factor = jnp.repeat(factor, TOK_DEV, axis=0)
    rough = jax.random.uniform(seed_list[4], (TOKENS, HEADS), jnp.float32, 0.2, 1.8)
    log_steps = -rates[None, :] * factor * rough
    places = jax.random.randint(seed_list[5], (3,), 0, TOKENS)
    losses = jnp.log(jax.random.uniform(seed_list[6], (3, HEADS), jnp.float32, 0.5, 0.8))
    log_steps = log_steps.at[places].add(jnp.where(slowly[None, :], losses, 0.0))
    return jnp.cumsum(log_steps, axis=0)


def block_levels(rng, dims, pieces, smallest, high):
    factor_of, own = 1.0, jax.random.fold_in(rng, 6)
    for dim, parts in pieces:
        heights = jnp.exp(jax.random.uniform(jax.random.fold_in(own, dim), (parts,), jnp.float32, smallest / len(pieces), high / len(pieces)))
        factor_of = factor_of * jnp.repeat(heights, dims[dim] // parts).reshape([-1 if axis == dim else 1 for axis in range(len(dims))])
    return factor_of


def assign_block(own_key, own, number, rows, count, top, most, skew):
    sequence = jax.random.permutation(own_key, count)
    crowded, common = load_shares(count, rows * top, most, skew, True), load_shares(count, rows * top, most, skew, False)
    places = jnp.arange(count)

    def named(lengths, rotation):
        used = int((lengths > 0).sum())
        fixed = max(1, used // 4)
        moved = fixed + (places - fixed + rotation * (used - fixed)) % max(1, count - fixed)
        return jnp.zeros((count,), jnp.int32).at[sequence[jnp.where(places < fixed, places, moved)]].set(jnp.asarray(lengths, jnp.int32))

    lengths = jnp.where(number % 4 == 0, named(crowded, number // 4), named(common, number - number // 4 - 1))
    mixed = jax.random.permutation(jax.random.fold_in(own, 3), count)
    source_of, receiver = mixed[0:count // 2 * 2:2], mixed[1:count // 2 * 2:2]
    margin = jnp.minimum(lengths[source_of] - 1, most - lengths[receiver]) // 2
    margin = jnp.where((source_of == sequence[0]) | (receiver == sequence[0]) | (lengths[receiver] == 0), 0, jnp.maximum(margin, 0))
    moved = jax.random.randint(jax.random.fold_in(own, 4), (count // 2,), 0, 1 << 20) % (margin + 1)
    lengths = lengths.at[source_of].add(-moved).at[receiver].add(moved)
    labels = jnp.searchsorted(jnp.cumsum(lengths), jnp.arange(rows * top), side="right").astype(jnp.int32)
    grid = labels.reshape(top, rows).T
    grid = grid[jax.random.permutation(jax.random.fold_in(own, 1), rows)]
    rotation = jax.random.randint(jax.random.fold_in(own, 2), (rows, 1), 0, top)
    return jnp.take_along_axis(grid, (jnp.arange(top)[None, :] + rotation) % top, axis=1)


def load_shares(count, total, reach, lean, full):
    weights = [(1 << 20) // math.isqrt(grade ** lean) + 1 for grade in range(1, count + 1)]
    largest = reach if full else min(reach, max(-(-total // count), total * weights[0] // sum(weights)))
    least = 1 if total - largest >= count - 1 else 0
    given, surplus = [largest] + [least] * (count - 1), total - largest - least * (count - 1)
    while surplus > 0:
        free = [i for i in range(1, count) if given[i] < largest] or [i for i in range(1, count) if given[i] < reach]
        whole, budget = sum([weights[i] for i in free]), surplus
        for i in free:
            more = min(reach - given[i], max(1, budget * weights[i] // whole), surplus)
            given[i] = given[i] + more
            surplus = surplus - more
    return np.array(given)


def scatter_about(own_key, extent, scale, limit, cuts=(), held_as=jnp.bfloat16):
    values = scale * jax.random.normal(own_key, extent, jnp.float32)
    if cuts:
        values = values * block_levels(own_key, extent, cuts, -0.22, 0.18)
    return jnp.clip(values, -limit, limit).astype(held_as)


def setup_inputs(seed: int = 0) -> dict:
    splits = jax.random.split(jax.random.key(seed), 16)
    residual = scatter_about(splits[0], (TOKENS, D), 1.0, 6.0, ((0, 32),))
    queries = draw_queries(jax.random.fold_in(splits[15], 71), 0)
    key_rows = draw_key_rows(jax.random.fold_in(splits[15], 71), 0)
    value_rows = scatter_about(splits[3], (TOKENS, KV_HEADS * HEAD_DIM), 1.0, 6.0, ((0, 8), (1, 4)))
    forget_sums = draw_forget_sums(jax.random.fold_in(splits[15], 71), 0)
    out_weight = scatter_about(splits[5], (HEADS * HEAD_DIM, D), (HEADS * HEAD_DIM // 4) ** -0.5, 0.25, ((0, 4),))
    norm_gain = jnp.clip(1.0 + 0.18 * jax.random.normal(splits[6], (D,), jnp.float32), 0.1, 1.9)
    expert_ids_keys = jax.random.split(jax.random.fold_in(splits[7], 1), TOKENS // ROWS)
    expert_ids_turns = jax.random.permutation(jax.random.fold_in(splits[7], 3), TOKENS // ROWS)
    expert_ids = jax.vmap(lambda own, number: assign_block(jax.random.fold_in(splits[7], 2), own, number, ROWS, EXPERTS, TOPK, CAP, 2))(expert_ids_keys, expert_ids_turns).reshape((TOKENS, TOPK))
    route_weights = jnp.clip(jnp.exp(math.log(1.0) - 2.3025851 * jax.random.uniform(splits[8], (TOKENS, TOPK), jnp.float32) ** block_levels(splits[8], (TOKENS, TOPK), ((0, 32),), -0.2, 0.2)), 0.1, 1.0)
    expert_gate = scatter_about(splits[9], (EXPERTS, D, FE), D ** -0.5, 0.125, ((0, 8),))
    expert_up = scatter_about(splits[10], (EXPERTS, D, FE), D ** -0.5, 0.125, ((0, 8),))
    expert_down = scatter_about(splits[11], (EXPERTS, FE, D), FE ** -0.5, 0.3125, ((0, 8),))
    shared_gate = scatter_about(splits[12], (D, FS), D ** -0.5, 0.125)
    shared_up = scatter_about(splits[13], (D, FS), D ** -0.5, 0.125)
    shared_down = scatter_about(splits[14], (FS, D), FS ** -0.5, 0.3125)
    return {"residual": residual, "queries": queries, "key_rows": key_rows, "value_rows": value_rows, "forget_sums": forget_sums, "out_weight": out_weight, "norm_gain": norm_gain, "expert_ids": expert_ids, "route_weights": route_weights, "expert_gate": expert_gate, "expert_up": expert_up, "expert_down": expert_down, "shared_gate": shared_gate, "shared_up": shared_up, "shared_down": shared_down}


routed_scale = 2.5
norm_eps = 1e-06

def attend(queries, key_rows, value_rows, forget_sums):
    group_size = HEADS // KV_HEADS
    score_scale = HEAD_DIM ** (-0.5)
    key_heads = key_rows.astype(jnp.float32).reshape(TOKENS, KV_HEADS, HEAD_DIM)
    value_heads = value_rows.astype(jnp.float32).reshape(TOKENS, KV_HEADS, HEAD_DIM)
    key_sums = forget_sums.reshape(TOKENS, KV_HEADS, group_size).transpose(1, 2, 0)
    positions = jnp.arange(TOKENS, dtype=jnp.int32)
    block_rows = math.gcd(TOKENS, 256)

    def one_block(first_pos):
        query_block = lax.dynamic_slice_in_dim(queries, first_pos, block_rows, 0).astype(jnp.float32)
        query_block = query_block.reshape(block_rows, KV_HEADS, group_size, HEAD_DIM)
        query_sums = lax.dynamic_slice_in_dim(forget_sums, first_pos, block_rows, 0)
        query_sums = query_sums.reshape(block_rows, KV_HEADS, group_size).transpose(1, 2, 0)
        scores = jnp.einsum('qhgd,khd->hgqk', query_block, key_heads) * score_scale
        scores = scores + (query_sums[:, :, :, None] - key_sums[:, :, None, :])
        query_pos = first_pos + jnp.arange(block_rows, dtype=jnp.int32)
        allowed = query_pos[:, None] >= positions[None, :]
        scores = jnp.where(allowed, scores, -jnp.inf)
        row_max = lax.optimization_barrier(jnp.max(scores, axis=3, keepdims=True))
        weights = jnp.exp(scores - row_max)
        weight_sum = lax.optimization_barrier(jnp.sum(weights, axis=3))
        rounded = lax.optimization_barrier(weights.astype(jnp.bfloat16)).astype(jnp.float32)
        mixed = jnp.einsum('hgqk,khd->qhgd', rounded, value_heads)
        mixed = mixed / weight_sum.transpose(2, 0, 1)[:, :, :, None]
        return mixed.reshape(block_rows, HEADS * HEAD_DIM).astype(jnp.bfloat16)
    starts = jnp.arange(TOKENS // block_rows, dtype=jnp.int32) * block_rows
    return lax.map(one_block, starts).reshape(TOKENS, HEADS * HEAD_DIM)

def experts_all(normed, expert_ids, route_weights, expert_gate, expert_up, expert_down):
    slot_count = TOKENS // ROWS * CAP
    flat_ids = expert_ids.reshape(-1)
    assigned = flat_ids.shape[0]
    gates = route_weights / lax.optimization_barrier(jnp.sum(route_weights, axis=1, keepdims=True)) * routed_scale
    flat_gates = jnp.concatenate([gates.reshape(-1), jnp.zeros((1,), jnp.float32)])
    padded = jnp.concatenate([normed, jnp.zeros((1, D), jnp.bfloat16)])

    def one_expert(carried, expert):
        chosen = flat_ids == expert
        place = jnp.where(chosen, jnp.cumsum(chosen.astype(jnp.int32)) - 1, slot_count)
        source = jnp.full((slot_count + 1,), assigned, jnp.int32)
        source = source.at[place].set(jnp.arange(assigned, dtype=jnp.int32))[:slot_count]
        token_rows = padded[source // TOPK]
        gate_part = jnp.dot(token_rows, expert_gate[expert], preferred_element_type=jnp.float32)
        up_part = jnp.dot(token_rows, expert_up[expert], preferred_element_type=jnp.float32)
        hidden = (jax.nn.silu(gate_part) * up_part).astype(jnp.bfloat16)
        output = jnp.dot(hidden, expert_down[expert], preferred_element_type=jnp.float32).astype(jnp.bfloat16)
        carried = carried.at[source // TOPK].add(flat_gates[source][:, None] * output.astype(jnp.float32))
        return (carried, None)
    routed, _ = lax.scan(one_expert, jnp.zeros((TOKENS + 1, D), jnp.float32), jnp.arange(EXPERTS, dtype=jnp.int32))
    return routed[:TOKENS]

def reference(residual, queries, key_rows, value_rows, forget_sums, out_weight, norm_gain, expert_ids, route_weights, expert_gate, expert_up, expert_down, shared_gate, shared_up, shared_down):
    attended = attend(queries, key_rows, value_rows, forget_sums)
    branch = jnp.dot(attended, out_weight, preferred_element_type=jnp.float32)
    stream = (residual.astype(jnp.float32) + branch).astype(jnp.bfloat16)
    wide = lax.optimization_barrier(stream).astype(jnp.float32)
    normed = (wide * lax.rsqrt(lax.optimization_barrier(jnp.mean(wide * wide, axis=1, keepdims=True)) + norm_eps) * norm_gain).astype(jnp.bfloat16)
    routed = experts_all(normed, expert_ids, route_weights, expert_gate, expert_up, expert_down)
    shared_hidden = (jax.nn.silu(jnp.dot(normed, shared_gate, preferred_element_type=jnp.float32)) * jnp.dot(normed, shared_up, preferred_element_type=jnp.float32)).astype(jnp.bfloat16)
    shared_out = jnp.dot(shared_hidden, shared_down, preferred_element_type=jnp.float32)
    return (wide + shared_out + routed).astype(jnp.bfloat16)
```

```python
import functools
import math

import jax
import jax.numpy as jnp
from jax import lax
from jax.experimental import pallas as pl
from jax.experimental.pallas import tpu as pltpu
from jax.sharding import PartitionSpec as P

HEADS = 16
KV_HEADS = 8
HEAD_DIM = 128
TOPK = 4


routed_scale = 2.5
norm_eps = 1e-06


MESH_ID = pl.DeviceIdType.MESH
LOG2E = math.log2(math.e)


def remote(src, dst, send_sem, recv_sem, target):
    return pltpu.make_async_remote_copy(
        src_ref=src,
        dst_ref=dst,
        send_sem=send_sem,
        recv_sem=recv_sem,
        device_id=target,
        device_id_type=MESH_ID,
    )


def greet(barrier, target):
    pl.semaphore_signal(barrier, inc=1, device_id=target, device_id_type=MESH_ID)


def attend_kernel(
    sp_count,
    score_scale,
    q_ref,
    fq_ref,
    k_hbm,
    v_hbm,
    fk_hbm,
    out_ref,
    kbuf,
    vbuf,
    fbuf,
    qs,
    acc,
    top,
    den,
    load_sem,
    up_sem,
    side_sem,
    recv_sem,
):
    me, tp = lax.axis_index("sp"), lax.axis_index("tp")
    line = sp_count // 2
    z, y = me // 2, me % 2
    mate = (2 * z + 1 - y, tp)
    above = (jnp.minimum(me + 2, sp_count - 1), tp)
    below = (jnp.maximum(me - 2, 0), tp)
    bufs = (kbuf, vbuf, fbuf)
    loads = [
        pltpu.make_async_copy(src, buf.at[me], load_sem.at[i])
        for i, (src, buf) in enumerate(zip((k_hbm, v_hbm, fk_hbm), bufs))
    ]
    for copy in loads:
        copy.start()
    barrier = pltpu.get_barrier_semaphore()
    greet(barrier, mate)

    @pl.when(z < line - 1)
    def _():
        greet(barrier, above)

    @pl.when(z > 0)
    def _():
        greet(barrier, below)

    rows, pair = q_ref.shape[0], qs.shape[1] // q_ref.shape[0]
    kv_heads = qs.shape[0]
    for h in range(kv_heads * pair):
        qs[h // pair, (h % pair) * rows : (h % pair + 1) * rows, :] = q_ref[
            :, h * HEAD_DIM : (h + 1) * HEAD_DIM
        ]
    for copy in loads:
        copy.wait()
    neighbours = 1 + (z < line - 1).astype(jnp.int32) + (z > 0).astype(jnp.int32)
    pl.semaphore_wait(barrier, neighbours)

    def moves(block, step, sems, target):
        return [
            remote(buf.at[block], buf.at[block], sems.at[step, i], recv_sem.at[block, i], target)
            for i, buf in enumerate(bufs)
        ]

    def forward(step):
        block = 2 * (z - step) + y

        @pl.when(z < line - 1)
        def _():
            for copy in moves(block, step, up_sem, above):
                copy.start()

        @pl.when(jnp.logical_or(y == 0, step > 0))
        def _():
            for copy in moves(block, step, side_sem, mate):
                copy.start()

    def absorb(block, first):
        for g in range(kv_heads):
            lanes = slice(g * HEAD_DIM, (g + 1) * HEAD_DIM)
            keys, values = kbuf[block, :, lanes], vbuf[block, :, lanes]
            products = lax.dot_general(
                qs[g], keys, (((1,), (1,)), ((), ())), preferred_element_type=jnp.float32
            )
            parts = []
            for j in range(pair):
                h = g * pair + j
                drop = fq_ref[:, h : h + 1] - fbuf[block, h : h + 1, :]
                part = products[j * rows : (j + 1) * rows] * (score_scale * LOG2E) + drop * LOG2E
                if first:
                    at_row = lax.broadcasted_iota(jnp.int32, part.shape, 0)
                    at_col = lax.broadcasted_iota(jnp.int32, part.shape, 1)
                    part = jnp.where(at_row >= at_col, part, -jnp.inf)
                parts.append(part)
            scores = jnp.concatenate(parts, axis=0)
            peak = jnp.max(scores, axis=1, keepdims=True)
            if first:
                weights = jnp.exp2(scores - peak)
                total = jnp.sum(weights, axis=1, keepdims=True)
            else:
                old = top[g][:, :1]
                peak = jnp.maximum(old, peak)
                factor = jnp.exp2(old - peak)
                weights = jnp.exp2(scores - peak)
                total = den[g][:, :1] * factor + jnp.sum(weights, axis=1, keepdims=True)
            mixed = jnp.dot(weights.astype(jnp.bfloat16), values, preferred_element_type=jnp.float32)
            acc[g] = mixed if first else acc[g] * factor + mixed
            top[g] = jnp.broadcast_to(peak, top.shape[1:])
            den[g] = jnp.broadcast_to(total, den.shape[1:])

    forward(0)
    absorb(me, True)

    def one_step(step, _):
        @pl.when(step <= z)
        def _():
            block = 2 * (z - step) + y
            for copy in moves(block, step, up_sem, below):
                copy.wait_recv()
            forward(step)
            absorb(block, False)

        @pl.when(jnp.logical_and(step - 1 <= z, jnp.logical_or(y == 1, step > 1)))
        def _():
            block = 2 * (z - step + 1) + 1 - y
            for copy in moves(block, step - 1, side_sem, mate):
                copy.wait_recv()
            absorb(block, False)

        return 0

    lax.fori_loop(1, line + 1, one_step, 0)
    for g in range(kv_heads):
        done = (acc[g] / den[g]).astype(jnp.bfloat16)
        for j in range(pair):
            h = g * pair + j
            out_ref[:, h * HEAD_DIM : (h + 1) * HEAD_DIM] = done[j * rows : (j + 1) * rows]

    def drain(step, _):
        @pl.when(step <= z)
        def _():
            block = 2 * (z - step) + y

            @pl.when(z < line - 1)
            def _():
                for copy in moves(block, step, up_sem, above):
                    copy.wait_send()

            @pl.when(jnp.logical_or(y == 0, step > 0))
            def _():
                for copy in moves(block, step, side_sem, mate):
                    copy.wait_send()

        return 0

    lax.fori_loop(0, line, drain, 0)


def attend_fused(queries, key_rows, value_rows, forget_sums, sp_count):
    rows, width = queries.shape
    kv_heads = key_rows.shape[1] // HEAD_DIM
    heads = width // HEAD_DIM
    key_sums = jnp.pad(forget_sums.T, ((0, 8 - heads), (0, 0)))
    line = sp_count // 2
    stacked = (kv_heads, heads // kv_heads * rows, HEAD_DIM)
    vmem, hbm = pl.BlockSpec(memory_space=pltpu.VMEM), pl.BlockSpec(memory_space=pl.ANY)
    return pl.pallas_call(
        functools.partial(attend_kernel, sp_count, HEAD_DIM ** (-0.5)),
        out_shape=jax.ShapeDtypeStruct((rows, width), jnp.bfloat16),
        in_specs=[vmem, vmem, hbm, hbm, hbm],
        out_specs=vmem,
        scratch_shapes=[
            pltpu.VMEM((sp_count,) + key_rows.shape, jnp.bfloat16),
            pltpu.VMEM((sp_count,) + value_rows.shape, jnp.bfloat16),
            pltpu.VMEM((sp_count,) + key_sums.shape, jnp.float32),
            pltpu.VMEM(stacked, jnp.bfloat16),
            pltpu.VMEM(stacked, jnp.float32),
            pltpu.VMEM(stacked, jnp.float32),
            pltpu.VMEM(stacked, jnp.float32),
            pltpu.SemaphoreType.DMA((3,)),
            pltpu.SemaphoreType.DMA((line, 3)),
            pltpu.SemaphoreType.DMA((line, 3)),
            pltpu.SemaphoreType.DMA((sp_count, 3)),
        ],
        compiler_params=pltpu.CompilerParams(
            collective_id=0, has_side_effects=True, vmem_limit_bytes=60 * 2**20
        ),
    )(queries, forget_sums, key_rows, value_rows, key_sums)


def tail_kernel(
    sp_count,
    att_ref,
    res_ref,
    gain_ref,
    gate_hbm,
    wo_hbm,
    eg_hbm,
    eu_hbm,
    ed_hbm,
    sg_hbm,
    su_hbm,
    sd_hbm,
    out_ref,
    wo,
    eg,
    eu,
    ed,
    sg,
    su,
    sd,
    gate_in,
    gate_buf,
    core_out,
    core_in,
    kept,
    x_out,
    x_in,
    base,
    tok,
    side_out,
    side_in,
    own,
    up_out,
    up_in,
    dn_out,
    dn_in,
    load_sem,
    gsend_sem,
    grecv_sem,
    pair_sem,
    hop_sem,
    tok_sem,
    side_send,
    side_recv,
    up_send,
    up_recv,
    dn_send,
    dn_recv,
):
    me, tp = lax.axis_index("sp"), lax.axis_index("tp")
    line = sp_count // 2
    z, y = me // 2, me % 2
    x, c = tp // 2, tp % 2
    mate = (2 * z + 1 - y, tp)
    above = (jnp.minimum(me + 2, sp_count - 1), tp)
    below = (jnp.maximum(me - 2, 0), tp)
    core_mate = (me, 2 * x + 1 - c)
    x_mate = (me, 2 * (1 - x) + c)
    rows = res_ref.shape[0]
    weights = [
        pltpu.make_async_copy(src, dst, load_sem.at[i])
        for i, (src, dst) in enumerate(
            (
                (gate_hbm, gate_in),
                (wo_hbm, wo),
                (sg_hbm, sg),
                (su_hbm, su),
                (sd_hbm, sd),
                (eg_hbm, eg),
                (eu_hbm, eu),
                (ed_hbm, ed),
            )
        )
    ]
    for copy in weights:
        copy.start()
    barrier = pltpu.get_barrier_semaphore()
    greet(barrier, core_mate)
    greet(barrier, x_mate)
    for j in range(1, sp_count):
        greet(barrier, (lax.rem(me + j, sp_count), tp))
    weights[0].wait()
    weights[1].wait()
    pl.semaphore_wait(barrier, sp_count + 1)

    def gate_move(j):
        peer, source = lax.rem(me + j, sp_count), me
        return remote(
            gate_in.at[peer], gate_buf.at[source], gsend_sem.at[j - 1], grecv_sem.at[j - 1], (peer, tp)
        )

    def gate_arrival(j):
        source = lax.rem(me - j + sp_count, sp_count)
        return remote(
            gate_in.at[source], gate_buf.at[source], gsend_sem.at[j - 1], grecv_sem.at[j - 1], (source, tp)
        )

    for j in range(1, sp_count):
        gate_move(j).start()

    far, near = (1 - x) * 2, x * 2

    def project(block):
        return jnp.dot(
            att_ref[pl.ds(pl.multiple_of(block * rows, rows), rows), :],
            wo[...],
            preferred_element_type=jnp.float32,
        )

    def project_to(i, _):
        out_x = jnp.where(i % 2 == 0, far, near)

        @pl.when(i < 2)
        def _():
            core_out[i % 2] = project(out_x + 1 - c).astype(jnp.bfloat16)
            remote(
                core_out.at[i % 2], core_in.at[i % 2], pair_sem.at[0, i % 2], pair_sem.at[1, i % 2], core_mate
            ).start()

        @pl.when(i >= 2)
        def _():
            kept[i % 2] = project(out_x + c)

        return 0

    lax.fori_loop(0, 4, project_to, 0)

    def core_copy(i):
        return remote(core_out.at[i], core_in.at[i], pair_sem.at[0, i], pair_sem.at[1, i], core_mate)

    core_copy(0).wait_recv()
    x_out[...] = (kept[0] + core_in[0].astype(jnp.float32)).astype(jnp.bfloat16)
    hop = remote(x_out, x_in, hop_sem.at[0], hop_sem.at[1], x_mate)
    hop.start()
    core_copy(1).wait_recv()
    branch = kept[1] + core_in[1].astype(jnp.float32) + res_ref[...].astype(jnp.float32)
    hop.wait_recv()
    stream = (branch + x_in[...].astype(jnp.float32)).astype(jnp.bfloat16)
    wide = stream.astype(jnp.float32)
    scale = lax.rsqrt(jnp.mean(wide * wide, axis=1, keepdims=True) + norm_eps)
    tok[me] = (wide * scale * gain_ref[...]).astype(jnp.bfloat16)
    base[...] = wide

    def tok_move(block, sem, target):
        return remote(tok.at[block], tok.at[block], sem, tok_sem.at[block], target)

    def block_of(where):
        return 2 * where + y

    def send_up(where):
        return tok_move(block_of(where), up_send.at[where], above)

    def send_dn(where):
        return tok_move(block_of(where), dn_send.at[where], below)

    def send_side(where):
        return tok_move(block_of(where), side_send.at[where], mate)

    send_side(z).start()

    @pl.when(z < line - 1)
    def _():
        send_up(z).start()

    @pl.when(z > 0)
    def _():
        send_dn(z).start()

    for copy in weights[2:]:
        copy.wait()

    def gated(inputs, gate, up, down):
        first = jnp.dot(inputs, gate[...], preferred_element_type=jnp.float32)
        second = jnp.dot(inputs, up[...], preferred_element_type=jnp.float32)
        hidden = (first / (1.0 + jnp.exp(-first)) * second).astype(jnp.bfloat16)
        return jnp.dot(hidden, down[...], preferred_element_type=jnp.float32)

    base[...] += gated(tok[me], sg, su, sd)
    for j in range(1, sp_count):
        gate_arrival(j).wait_recv()
    gate_buf[me] = gate_in[me]

    def expert(block):
        row = gate_buf[block][:1, :]
        shape = (rows, row.shape[1])
        diagonal = lax.broadcasted_iota(jnp.int32, shape, 0) == lax.broadcasted_iota(jnp.int32, shape, 1)
        column = jnp.sum(jnp.where(diagonal, row, 0.0), axis=1, keepdims=True)
        result = gated(tok[block], eg, eu, ed).astype(jnp.bfloat16).astype(jnp.float32)
        return result * column

    def side_back(where):
        return remote(
            side_out.at[where], side_in.at[where], side_send.at[line + where], side_recv.at[where], mate
        )

    def mates_block(where):
        tok_move(2 * where + 1 - y, side_send.at[where], mate).wait_recv()
        side_out[where] = expert(2 * where + 1 - y).astype(jnp.bfloat16)
        side_back(where).start()

    own[z] = expert(me)
    mates_block(z)

    def one_step(step, _):
        low, high = z - step, z + step

        @pl.when(low >= 0)
        def _():
            tok_move(block_of(low), up_send.at[low], below).wait_recv()
            send_side(low).start()

            @pl.when(z < line - 1)
            def _():
                send_up(low).start()

        @pl.when(high < line)
        def _():
            tok_move(block_of(high), dn_send.at[high], above).wait_recv()
            send_side(high).start()

            @pl.when(z > 0)
            def _():
                send_dn(high).start()

        def at(i, _):
            where = jnp.where(i == 0, low, high)

            @pl.when(jnp.logical_and(where >= 0, where < line))
            def _():
                own[where] = expert(block_of(where))

            return 0

        def at_mates(i, _):
            where = jnp.where(i == 0, low, high)

            @pl.when(jnp.logical_and(where >= 0, where < line))
            def _():
                mates_block(where)

            return 0

        lax.fori_loop(0, 2, at, 0)
        lax.fori_loop(0, 2, at_mates, 0)
        return 0

    lax.fori_loop(1, line, one_step, 0)

    def up_back(where):
        return remote(up_out.at[where], up_in.at[where], up_send.at[line + where], up_recv.at[where], above)

    def dn_back(where):
        return remote(dn_out.at[where], dn_in.at[where], dn_send.at[line + where], dn_recv.at[where], below)

    def back_step(turn, _):
        step = turn % (line - 1) + 1
        upward = (turn < line - 1) == (2 * z < line - 1)
        low, high = z - step, z + step

        @pl.when(jnp.logical_and(upward, high < line))
        def _():
            side_back(high).wait_recv()
            own[high] = own[high] + side_in[high].astype(jnp.float32)

            @pl.when(z > 0)
            def _():
                up_back(high).wait_recv()
                own[high] = own[high] + up_in[high].astype(jnp.float32)

            up_out[high] = own[high].astype(jnp.bfloat16)
            up_back(high).start()

        @pl.when(jnp.logical_and(jnp.logical_not(upward), low >= 0))
        def _():
            side_back(low).wait_recv()
            own[low] = own[low] + side_in[low].astype(jnp.float32)

            @pl.when(z < line - 1)
            def _():
                dn_back(low).wait_recv()
                own[low] = own[low] + dn_in[low].astype(jnp.float32)

            dn_out[low] = own[low].astype(jnp.bfloat16)
            dn_back(low).start()

        return 0

    lax.fori_loop(0, 2 * (line - 1), back_step, 0)
    side_back(z).wait_recv()
    base[...] += own[z] + side_in[z].astype(jnp.float32)

    @pl.when(z > 0)
    def _():
        up_back(z).wait_recv()
        base[...] += up_in[z].astype(jnp.float32)

    @pl.when(z < line - 1)
    def _():
        dn_back(z).wait_recv()
        base[...] += dn_in[z].astype(jnp.float32)

    out_ref[...] = base[...].astype(jnp.bfloat16)
    for j in range(1, sp_count):
        gate_move(j).wait_send()
    for i in range(2):
        core_copy(i).wait_send()
    hop.wait_send()

    def drain(where, _):
        send_side(where).wait_send()
        side_back(where).wait_send()

        @pl.when(jnp.logical_and(where <= z, z < line - 1))
        def _():
            send_up(where).wait_send()

        @pl.when(jnp.logical_and(where >= z, z > 0))
        def _():
            send_dn(where).wait_send()

        @pl.when(where > z)
        def _():
            up_back(where).wait_send()

        @pl.when(where < z)
        def _():
            dn_back(where).wait_send()

        return 0

    lax.fori_loop(0, line, drain, 0)


def tail_fused(
    attended,
    residual,
    norm_gain,
    expert_ids,
    route_weights,
    out_weight,
    expert_gate,
    expert_up,
    expert_down,
    shared_gate,
    shared_up,
    shared_down,
    sp_count,
):
    rows, width = residual.shape
    line = sp_count // 2
    gates = route_weights / jnp.sum(route_weights, axis=1, keepdims=True) * routed_scale
    named = expert_ids[None, :, :] == jnp.arange(sp_count, dtype=jnp.int32)[:, None, None]
    table = jnp.sum(jnp.where(named, gates[None], 0.0), axis=2)
    lanes = -(-rows // 128) * 128
    table = jnp.broadcast_to(
        jnp.pad(table, ((0, 0), (0, lanes - rows)))[:, None, :], (sp_count, 8, lanes)
    )
    vmem, hbm = pl.BlockSpec(memory_space=pltpu.VMEM), pl.BlockSpec(memory_space=pl.ANY)
    bf16, f32 = jnp.bfloat16, jnp.float32
    loaded = (
        out_weight,
        expert_gate[0],
        expert_up[0],
        expert_down[0],
        shared_gate,
        shared_up,
        shared_down,
    )
    dma = pltpu.SemaphoreType.DMA
    one = (rows, width)
    return pl.pallas_call(
        functools.partial(tail_kernel, sp_count),
        out_shape=jax.ShapeDtypeStruct(one, bf16),
        in_specs=[vmem, vmem, vmem] + [hbm] * 8,
        out_specs=vmem,
        scratch_shapes=[pltpu.VMEM(w.shape, bf16) for w in loaded]
        + [
            pltpu.VMEM(table.shape, f32),
            pltpu.VMEM(table.shape, f32),
            pltpu.VMEM((2,) + one, bf16),
            pltpu.VMEM((2,) + one, bf16),
            pltpu.VMEM((2,) + one, f32),
            pltpu.VMEM(one, bf16),
            pltpu.VMEM(one, bf16),
            pltpu.VMEM(one, f32),
            pltpu.VMEM((sp_count,) + one, bf16),
            pltpu.VMEM((line,) + one, bf16),
            pltpu.VMEM((line,) + one, bf16),
            pltpu.VMEM((line,) + one, f32),
            pltpu.VMEM((line,) + one, bf16),
            pltpu.VMEM((line,) + one, bf16),
            pltpu.VMEM((line,) + one, bf16),
            pltpu.VMEM((line,) + one, bf16),
            dma((8,)),
            dma((sp_count - 1,)),
            dma((sp_count - 1,)),
            dma((2, 2)),
            dma((2,)),
            dma((sp_count,)),
            dma((2 * line,)),
            dma((line,)),
            dma((2 * line,)),
            dma((line,)),
            dma((2 * line,)),
            dma((line,)),
        ],
        compiler_params=pltpu.CompilerParams(
            collective_id=1, has_side_effects=True, vmem_limit_bytes=60 * 2**20
        ),
    )(attended, residual, norm_gain[None, :], table, *loaded)


def absorb_group(carried, query_group, shard_piece, sum_piece, score_scale):
    query_heads, query_sums, query_pos, last_pos = query_group
    key_piece, value_piece = shard_piece
    piece_rows = key_piece.shape[0]
    query_count, local_kv, group_size, head_size = query_heads.shape
    key_block = math.gcd(piece_rows, 1024)
    key_heads = key_piece.reshape(piece_rows, local_kv, head_size)
    value_heads = value_piece.reshape(piece_rows, local_kv, head_size)
    key_sums = sum_piece.reshape(piece_rows, local_kv, group_size).transpose(1, 2, 0)

    def update(block_start, held):
        row_max, row_sum, weighted = held
        key_part = lax.dynamic_slice_in_dim(key_heads, block_start, key_block, 0)
        value_part = lax.dynamic_slice_in_dim(value_heads, block_start, key_block, 0)
        sums_part = lax.dynamic_slice_in_dim(key_sums, block_start, key_block, 2)
        scores = (
            jnp.einsum("qhgd,khd->hgqk", query_heads, key_part, preferred_element_type=jnp.float32)
            * score_scale
        )
        scores = scores + (query_sums[:, :, :, None] - sums_part[:, :, None, :])
        key_pos = block_start + jnp.arange(key_block, dtype=jnp.int32)
        allowed = query_pos[:, None] >= key_pos[None, :]
        scores = jnp.where(allowed, scores, -jnp.inf)
        new_max = jnp.maximum(row_max, jnp.max(scores, axis=3))
        weights = jnp.exp(scores - new_max[:, :, :, None])
        factor = jnp.exp(row_max - new_max)
        row_sum = row_sum * factor + jnp.sum(weights, axis=3)
        products = jnp.einsum(
            "hgqk,khd->qhgd",
            weights.astype(jnp.bfloat16),
            value_part,
            preferred_element_type=jnp.float32,
        )
        weighted = weighted * factor.transpose(2, 0, 1)[:, :, :, None] + products
        return (new_max, row_sum, weighted)

    def one_block(block_index, held):
        block_start = block_index * key_block
        needed = block_start <= last_pos
        return lax.cond(needed, lambda inner: update(block_start, inner), lambda inner: inner, held)

    return lax.fori_loop(0, piece_rows // key_block, one_block, carried)


def finish(carried):
    row_max, row_sum, weighted = carried
    mixed = weighted / row_sum.transpose(2, 0, 1)[:, :, :, None]
    return mixed.reshape(mixed.shape[0], -1).astype(jnp.bfloat16)


def local(
    residual,
    queries,
    key_rows,
    value_rows,
    forget_sums,
    out_weight,
    norm_gain,
    expert_ids,
    route_weights,
    expert_gate,
    expert_up,
    expert_down,
    shared_gate,
    shared_up,
    shared_down,
):
    sp_count = lax.axis_size("sp")
    sp_index = lax.axis_index("sp")
    local_rows = queries.shape[0]
    local_kv = key_rows.shape[1] // HEAD_DIM
    group_size = HEADS // KV_HEADS
    score_scale = HEAD_DIM ** (-0.5)
    tp_count = lax.axis_size("tp")
    tokens_here = residual.shape[0]
    every_slot = 2 * tokens_here * TOPK >= tokens_here * expert_gate.shape[0] * sp_count
    if every_slot and expert_gate.shape[0] == 1 and sp_count % 2 == 0 and tp_count == 4:
        attended = attend_fused(queries, key_rows, value_rows, forget_sums, sp_count)
        return tail_fused(
            attended,
            residual,
            norm_gain,
            expert_ids,
            route_weights,
            out_weight,
            expert_gate,
            expert_up,
            expert_down,
            shared_gate,
            shared_up,
            shared_down,
            sp_count,
        )
    own_first = sp_index * local_rows
    all_sums = lax.all_gather(forget_sums, "sp", axis=0, tiled=True)
    positions = own_first + jnp.arange(local_rows, dtype=jnp.int32)
    groups = [
        (
            queries.reshape(queries.shape[0], local_kv, group_size, HEAD_DIM),
            forget_sums.reshape(forget_sums.shape[0], local_kv, group_size).transpose(1, 2, 0),
            positions,
            positions[-1],
        )
    ]

    def initial(query_count):
        return (
            jnp.full((local_kv, group_size, query_count), -1e30, jnp.float32),
            jnp.zeros((local_kv, group_size, query_count), jnp.float32),
            jnp.zeros((query_count, local_kv, group_size, HEAD_DIM), jnp.float32),
        )

    def absorb(states, shard_piece):
        return tuple(
            (
                absorb_group(held, query_group, shard_piece, all_sums, score_scale)
                for held, query_group in zip(states, groups)
            )
        )

    start_states = tuple((initial(query_group[0].shape[0]) for query_group in groups))
    states = absorb(
        start_states,
        (
            lax.all_gather(key_rows, "sp", axis=0, tiled=True),
            lax.all_gather(value_rows, "sp", axis=0, tiled=True),
        ),
    )
    outputs = [finish(held) for held in states]
    attended = outputs[0]
    rows_out = local_rows // lax.axis_size("tp")
    branch = lax.psum_scatter(
        jnp.dot(attended, out_weight, preferred_element_type=jnp.float32).astype(jnp.bfloat16),
        "tp",
        scatter_dimension=0,
        tiled=True,
    ).astype(jnp.float32)
    stream = (residual.astype(jnp.float32) + branch).astype(jnp.bfloat16)
    wide = lax.optimization_barrier(stream).astype(jnp.float32)
    normed = (
        wide * lax.rsqrt(jnp.mean(wide * wide, axis=1, keepdims=True) + norm_eps) * norm_gain
    ).astype(jnp.bfloat16)
    width = normed.shape[1]
    experts_here = expert_gate.shape[0]
    total_experts = experts_here * sp_count
    capacity = 2 * rows_out * TOPK // total_experts
    flat_ids = expert_ids.reshape(-1)
    assigned = flat_ids.shape[0]
    onehot = (flat_ids[:, None] == jnp.arange(total_experts, dtype=jnp.int32)[None, :]).astype(
        jnp.int32
    )
    slot_rank = jnp.sum((jnp.cumsum(onehot, axis=0) - 1) * onehot, axis=1)
    target = flat_ids * capacity + slot_rank
    slot_count = total_experts * capacity
    source = (
        jnp.full((slot_count,), assigned, jnp.int32)
        .at[target]
        .set(jnp.arange(assigned, dtype=jnp.int32))
    )
    padded = jnp.concatenate([normed, jnp.zeros((1, width), jnp.bfloat16)], axis=0)
    outgoing = padded[source // TOPK].reshape(sp_count, experts_here, capacity, width)
    arrived = lax.all_to_all(outgoing, "sp", split_axis=0, concat_axis=0, tiled=True)
    gate_part = jnp.einsum(
        "necd,edf->necf", arrived, expert_gate, preferred_element_type=jnp.float32
    )
    up_part = jnp.einsum("necd,edf->necf", arrived, expert_up, preferred_element_type=jnp.float32)
    hidden = (jax.nn.silu(gate_part) * up_part).astype(jnp.bfloat16)
    processed = jnp.einsum(
        "necf,efd->necd", hidden, expert_down, preferred_element_type=jnp.float32
    ).astype(jnp.bfloat16)
    returned = lax.all_to_all(processed, "sp", split_axis=0, concat_axis=0, tiled=True)
    results = returned.reshape(slot_count, width)
    picked = results[target].reshape(rows_out, TOPK, width).astype(jnp.float32)
    gates = route_weights / jnp.sum(route_weights, axis=1, keepdims=True) * routed_scale
    routed = jnp.sum(gates[:, :, None] * picked, axis=1)
    shared_hidden = (
        jax.nn.silu(jnp.dot(normed, shared_gate, preferred_element_type=jnp.float32))
        * jnp.dot(normed, shared_up, preferred_element_type=jnp.float32)
    ).astype(jnp.bfloat16)
    shared_out = jnp.dot(shared_hidden, shared_down, preferred_element_type=jnp.float32)
    return (wide + shared_out + routed).astype(jnp.bfloat16)


def solution(mesh):
    in_specs = (
        P(("sp", "tp"), None),
        P("sp", "tp"),
        P("sp", "tp"),
        P("sp", "tp"),
        P("sp", "tp"),
        P("tp", None),
        P(),
        P(("sp", "tp"), None),
        P(("sp", "tp"), None),
        P("sp", None, None),
        P("sp", None, None),
        P("sp", None, None),
        P(),
        P(),
        P(),
    )
    out_specs = P(("sp", "tp"), None)
    return jax.shard_map(local, mesh=mesh, in_specs=in_specs, out_specs=out_specs, check_vma=False)
```

```python
import functools
import math

import jax
import jax.numpy as jnp
from jax import lax
from jax.experimental import pallas as pl
from jax.experimental.pallas import tpu as pltpu
from jax.sharding import PartitionSpec as P

HEADS = 16
KV_HEADS = 8
HEAD_DIM = 128
TOPK = 4


routed_scale = 2.5
norm_eps = 1e-06


MESH_ID = pl.DeviceIdType.MESH
LOG2E = math.log2(math.e)


def remote(src, dst, send_sem, recv_sem, target):
    return pltpu.make_async_remote_copy(
        src_ref=src,
        dst_ref=dst,
        send_sem=send_sem,
        recv_sem=recv_sem,
        device_id=target,
        device_id_type=MESH_ID,
    )


def greet(barrier, target):
    pl.semaphore_signal(barrier, inc=1, device_id=target, device_id_type=MESH_ID)


def attend_kernel(
    sp_count,
    score_scale,
    q_ref,
    f_ref,
    k_hbm,
    v_hbm,
    out_ref,
    kbuf,
    vbuf,
    fbuf,
    qs,
    fqs,
    acc,
    top,
    den,
    load_sem,
    up_sem,
    side_sem,
    recv_sem,
):
    me, tp = lax.axis_index("sp"), lax.axis_index("tp")
    line = sp_count // 2
    z, y = me // 2, me % 2
    mate = (2 * z + 1 - y, tp)
    above = (jnp.minimum(me + 2, sp_count - 1), tp)
    below = (jnp.maximum(me - 2, 0), tp)
    bufs = (kbuf, vbuf, fbuf)
    loads = [
        pltpu.make_async_copy(src, buf.at[me], load_sem.at[i])
        for i, (src, buf) in enumerate(zip((k_hbm, v_hbm), bufs))
    ]
    for copy in loads:
        copy.start()
    fbuf[me] = jnp.zeros(fbuf.shape[1:], jnp.float32)
    fbuf[me, : f_ref.shape[0], :] = f_ref[...]
    barrier = pltpu.get_barrier_semaphore()
    greet(barrier, mate)

    @pl.when(z < line - 1)
    def _():
        greet(barrier, above)

    @pl.when(z > 0)
    def _():
        greet(barrier, below)

    rows, pair = q_ref.shape[0], qs.shape[1] // q_ref.shape[0]
    kv_heads = qs.shape[0]
    for h in range(kv_heads * pair):
        qs[h // pair, (h % pair) * rows : (h % pair + 1) * rows, :] = q_ref[
            :, h * HEAD_DIM : (h + 1) * HEAD_DIM
        ]
    square = (rows, rows)
    diagonal = lax.broadcasted_iota(jnp.int32, square, 0) == lax.broadcasted_iota(jnp.int32, square, 1)
    for h in range(kv_heads * pair):
        column = jnp.sum(jnp.where(diagonal, f_ref[h : h + 1, :], 0.0), axis=1, keepdims=True)
        fqs[h // pair, (h % pair) * rows : (h % pair + 1) * rows, :] = jnp.broadcast_to(
            column, (rows, HEAD_DIM)
        )
    for copy in loads:
        copy.wait()
    neighbours = 1 + (z < line - 1).astype(jnp.int32) + (z > 0).astype(jnp.int32)
    pl.semaphore_wait(barrier, neighbours)

    def moves(block, step, sems, target):
        return [
            remote(buf.at[block], buf.at[block], sems.at[step, i], recv_sem.at[block, i], target)
            for i, buf in enumerate(bufs)
        ]

    def forward(step, arriving):
        block = 2 * (z - step) + y
        for i in (2, 0, 1):
            if arriving:
                moves(block, step, up_sem, below)[i].wait_recv()

            @pl.when(z < line - 1)
            def _():
                moves(block, step, up_sem, above)[i].start()

            @pl.when(jnp.logical_or(y == 0, step > 0))
            def _():
                moves(block, step, side_sem, mate)[i].start()

    def absorb(block, first):
        for g in range(kv_heads):
            lanes = slice(g * HEAD_DIM, (g + 1) * HEAD_DIM)
            keys, values = kbuf[block, :, lanes], vbuf[block, :, lanes]
            products = lax.dot_general(
                qs[g], keys, (((1,), (1,)), ((), ())), preferred_element_type=jnp.float32
            )
            parts = []
            for j in range(pair):
                h = g * pair + j
                drop = fqs[g, j * rows : (j + 1) * rows, :1] - fbuf[block, h : h + 1, :]
                part = products[j * rows : (j + 1) * rows] * (score_scale * LOG2E) + drop * LOG2E
                if first:
                    at_row = lax.broadcasted_iota(jnp.int32, part.shape, 0)
                    at_col = lax.broadcasted_iota(jnp.int32, part.shape, 1)
                    part = jnp.where(at_row >= at_col, part, -jnp.inf)
                parts.append(part)
            scores = jnp.concatenate(parts, axis=0)
            peak = jnp.max(scores, axis=1, keepdims=True)
            if first:
                weights = jnp.exp2(scores - peak)
                total = jnp.sum(weights, axis=1, keepdims=True)
            else:
                old = top[g][:, :1]
                peak = jnp.maximum(old, peak)
                factor = jnp.exp2(old - peak)
                weights = jnp.exp2(scores - peak)
                total = den[g][:, :1] * factor + jnp.sum(weights, axis=1, keepdims=True)
            mixed = jnp.dot(weights.astype(jnp.bfloat16), values, preferred_element_type=jnp.float32)
            acc[g] = mixed if first else acc[g] * factor + mixed
            top[g] = jnp.broadcast_to(peak, top.shape[1:])
            den[g] = jnp.broadcast_to(total, den.shape[1:])

    forward(0, False)
    absorb(me, True)

    def one_step(step, _):
        @pl.when(step <= z)
        def _():
            block = 2 * (z - step) + y
            forward(step, True)
            absorb(block, False)

        @pl.when(jnp.logical_and(step - 1 <= z, jnp.logical_or(y == 1, step > 1)))
        def _():
            block = 2 * (z - step + 1) + 1 - y
            for copy in moves(block, step - 1, side_sem, mate):
                copy.wait_recv()
            absorb(block, False)

        return 0

    lax.fori_loop(1, line + 1, one_step, 0)
    for g in range(kv_heads):
        done = (acc[g] / den[g]).astype(jnp.bfloat16)
        for j in range(pair):
            h = g * pair + j
            out_ref[:, h * HEAD_DIM : (h + 1) * HEAD_DIM] = done[j * rows : (j + 1) * rows]

    def drain(step, _):
        @pl.when(step <= z)
        def _():
            block = 2 * (z - step) + y

            @pl.when(z < line - 1)
            def _():
                for copy in moves(block, step, up_sem, above):
                    copy.wait_send()

            @pl.when(jnp.logical_or(y == 0, step > 0))
            def _():
                for copy in moves(block, step, side_sem, mate):
                    copy.wait_send()

        return 0

    lax.fori_loop(0, line, drain, 0)


def attend_fused(queries, key_rows, value_rows, forget_sums, sp_count):
    rows, width = queries.shape
    kv_heads = key_rows.shape[1] // HEAD_DIM
    heads = width // HEAD_DIM
    line = sp_count // 2
    stacked = (kv_heads, heads // kv_heads * rows, HEAD_DIM)
    vmem, hbm = pl.BlockSpec(memory_space=pltpu.VMEM), pl.BlockSpec(memory_space=pl.ANY)
    return pl.pallas_call(
        functools.partial(attend_kernel, sp_count, HEAD_DIM ** (-0.5)),
        out_shape=jax.ShapeDtypeStruct((rows, width), jnp.bfloat16),
        in_specs=[vmem, vmem, hbm, hbm],
        out_specs=vmem,
        scratch_shapes=[
            pltpu.VMEM((sp_count,) + key_rows.shape, jnp.bfloat16),
            pltpu.VMEM((sp_count,) + value_rows.shape, jnp.bfloat16),
            pltpu.VMEM((sp_count, -(-heads // 8) * 8, rows), jnp.float32),
            pltpu.VMEM(stacked, jnp.bfloat16),
            pltpu.VMEM(stacked, jnp.float32),
            pltpu.VMEM(stacked, jnp.float32),
            pltpu.VMEM(stacked, jnp.float32),
            pltpu.VMEM(stacked, jnp.float32),
            pltpu.SemaphoreType.DMA((2,)),
            pltpu.SemaphoreType.DMA((line, 3)),
            pltpu.SemaphoreType.DMA((line, 3)),
            pltpu.SemaphoreType.DMA((sp_count, 3)),
        ],
        compiler_params=pltpu.CompilerParams(
            collective_id=0, has_side_effects=True, vmem_limit_bytes=60 * 2**20
        ),
    )(queries, forget_sums.T, key_rows, value_rows)


def tail_kernel(
    sp_count,
    att_ref,
    res_ref,
    gain_ref,
    ids_ref,
    score_ref,
    wo_hbm,
    eg_hbm,
    eu_hbm,
    ed_hbm,
    sg_hbm,
    su_hbm,
    sd_hbm,
    out_ref,
    wo,
    eg,
    eu,
    ed,
    sg,
    su,
    sd,
    gate_in,
    gate_buf,
    core_out,
    core_in,
    kept,
    x_out,
    x_in,
    base,
    tok,
    side_out,
    side_in,
    own,
    up_out,
    up_in,
    dn_out,
    dn_in,
    load_sem,
    gsend_sem,
    grecv_sem,
    pair_sem,
    hop_sem,
    tok_sem,
    side_send,
    side_recv,
    up_send,
    up_recv,
    dn_send,
    dn_recv,
):
    me, tp = lax.axis_index("sp"), lax.axis_index("tp")
    line = sp_count // 2
    z, y = me // 2, me % 2
    x, c = tp // 2, tp % 2
    mate = (2 * z + 1 - y, tp)
    above = (jnp.minimum(me + 2, sp_count - 1), tp)
    below = (jnp.maximum(me - 2, 0), tp)
    core_mate = (me, 2 * x + 1 - c)
    x_mate = (me, 2 * (1 - x) + c)
    rows = res_ref.shape[0]
    weights = [
        pltpu.make_async_copy(src, dst, load_sem.at[i])
        for i, (src, dst) in enumerate(
            (
                (wo_hbm, wo),
                (sg_hbm, sg),
                (su_hbm, su),
                (sd_hbm, sd),
                (eg_hbm, eg),
                (eu_hbm, eu),
                (ed_hbm, ed),
            )
        )
    ]
    for copy in weights:
        copy.start()
    barrier = pltpu.get_barrier_semaphore()
    greet(barrier, core_mate)
    greet(barrier, x_mate)
    for j in range(1, sp_count):
        greet(barrier, (lax.rem(me + j, sp_count), tp))
    scores = score_ref[...]
    gates = scores / jnp.sum(scores, axis=0, keepdims=True) * routed_scale
    for e in range(sp_count):
        row = jnp.sum(jnp.where(ids_ref[...] == e, gates, 0.0), axis=0, keepdims=True)
        gate_in[e] = jnp.broadcast_to(row, gate_in.shape[1:])
    weights[0].wait()
    pl.semaphore_wait(barrier, sp_count + 1)

    def gate_move(j):
        peer, source = lax.rem(me + j, sp_count), me
        return remote(
            gate_in.at[peer], gate_buf.at[source], gsend_sem.at[j - 1], grecv_sem.at[j - 1], (peer, tp)
        )

    def gate_arrival(j):
        source = lax.rem(me - j + sp_count, sp_count)
        return remote(
            gate_in.at[source], gate_buf.at[source], gsend_sem.at[j - 1], grecv_sem.at[j - 1], (source, tp)
        )

    for j in range(1, sp_count):
        gate_move(j).start()

    far, near = (1 - x) * 2, x * 2

    def core_copy(i):
        return remote(core_out.at[i], core_in.at[i], pair_sem.at[0, i], pair_sem.at[1, i], core_mate)

    hop = remote(x_out, x_in, hop_sem.at[0], hop_sem.at[1], x_mate)

    def project(block):
        return jnp.dot(
            att_ref[pl.ds(pl.multiple_of(block * rows, rows), rows), :],
            wo[...],
            preferred_element_type=jnp.float32,
        )

    def project_to(i, _):
        out_x = jnp.where(i == 0, far, near)
        core_out[i] = project(out_x + 1 - c).astype(jnp.bfloat16)
        core_copy(i).start()
        kept[i] = project(out_x + c)
        core_copy(i).wait_recv()
        kept[i] = kept[i] + core_in[i].astype(jnp.float32)

        @pl.when(i == 0)
        def _():
            x_out[...] = kept[0].astype(jnp.bfloat16)
            hop.start()

        return 0

    lax.fori_loop(0, 2, project_to, 0)
    branch = kept[1] + res_ref[...].astype(jnp.float32)
    hop.wait_recv()
    stream = (branch + x_in[...].astype(jnp.float32)).astype(jnp.bfloat16)
    wide = stream.astype(jnp.float32)
    scale = lax.rsqrt(jnp.mean(wide * wide, axis=1, keepdims=True) + norm_eps)
    tok[me] = (wide * scale * gain_ref[...]).astype(jnp.bfloat16)
    base[...] = wide

    halves = 2
    part_rows = rows // halves

    def piece(ref, i, p):
        return ref.at[i, pl.ds(p * part_rows, part_rows), :]

    def tok_move(block, p, sem, target):
        return remote(piece(tok, block, p), piece(tok, block, p), sem, tok_sem.at[block, p], target)

    def block_of(where):
        return 2 * where + y

    def send_up(where, p):
        return tok_move(block_of(where), p, up_send.at[where, p], above)

    def send_dn(where, p):
        return tok_move(block_of(where), p, dn_send.at[where, p], below)

    def send_side(where, p):
        return tok_move(block_of(where), p, side_send.at[where, p], mate)

    for p in range(halves):
        send_side(z, p).start()

        @pl.when(z < line - 1)
        def _():
            send_up(z, p).start()

        @pl.when(z > 0)
        def _():
            send_dn(z, p).start()

    for copy in weights[1:]:
        copy.wait()

    def gated(inputs, gate, up, down):
        first = jnp.dot(inputs, gate[...], preferred_element_type=jnp.float32)
        second = jnp.dot(inputs, up[...], preferred_element_type=jnp.float32)
        hidden = (first / (1.0 + jnp.exp(-first)) * second).astype(jnp.bfloat16)
        return jnp.dot(hidden, down[...], preferred_element_type=jnp.float32)

    base[...] += gated(tok[me], sg, su, sd)
    for j in range(1, sp_count):
        gate_arrival(j).wait_recv()
    gate_buf[me] = gate_in[me]

    def expert(block):
        row = gate_buf[block][:1, :]
        shape = (rows, row.shape[1])
        diagonal = lax.broadcasted_iota(jnp.int32, shape, 0) == lax.broadcasted_iota(jnp.int32, shape, 1)
        column = jnp.sum(jnp.where(diagonal, row, 0.0), axis=1, keepdims=True)
        result = gated(tok[block], eg, eu, ed).astype(jnp.bfloat16).astype(jnp.float32)
        return result * column

    def side_back(where, p):
        return remote(
            piece(side_out, where, p),
            piece(side_in, where, p),
            side_send.at[line + where, p],
            side_recv.at[where, p],
            mate,
        )

    def inside(where):
        return jnp.logical_and(where >= 0, where < line)

    def mates_block(where):
        for p in range(halves):
            tok_move(2 * where + 1 - y, p, side_send.at[where, p], mate).wait_recv()
        side_out[where] = expert(2 * where + 1 - y).astype(jnp.bfloat16)

    def own_part(step):
        def at(i, _):
            where = jnp.where(i == 0, z - step, z + step)

            @pl.when(inside(where))
            def _():
                own[where] = expert(block_of(where))

            return 0

        lax.fori_loop(0, 2, at, 0)

    def mates_part(step):
        def at(i, _):
            where = jnp.where(i == 0, z - step, z + step)

            @pl.when(jnp.logical_and(inside(where), jnp.logical_or(i == 0, step > 0)))
            def _():
                mates_block(where)

            return 0

        lax.fori_loop(0, 2, at, 0)

    own[z] = expert(me)

    def one_step(step, _):
        low, high = z - step, z + step
        for p in range(halves):

            @pl.when(low >= 0)
            def _():
                tok_move(block_of(low), p, up_send.at[low, p], below).wait_recv()
                send_side(low, p).start()

                @pl.when(z < line - 1)
                def _():
                    send_up(low, p).start()

            @pl.when(high < line)
            def _():
                tok_move(block_of(high), p, dn_send.at[high, p], above).wait_recv()
                send_side(high, p).start()

                @pl.when(z > 0)
                def _():
                    send_dn(high, p).start()

        @pl.when(step == line - 1)
        def _():
            for p in range(halves):
                side_back(z, p).start()

        own_part(step)
        mates_part(step - 1)
        return 0

    lax.fori_loop(1, line, one_step, 0)
    mates_part(line - 1)

    def cross(turn, _):
        step = line - 1 - turn
        for where in (z - step, z + step):

            @pl.when(inside(where))
            def _():
                for p in range(halves):
                    side_back(where, p).start()

        return 0

    lax.fori_loop(0, line - 1, cross, 0)

    def up_back(where, p):
        return remote(
            piece(up_out, where, p),
            piece(up_in, where, p),
            up_send.at[line + where, p],
            up_recv.at[where, p],
            above,
        )

    def dn_back(where, p):
        return remote(
            piece(dn_out, where, p),
            piece(dn_in, where, p),
            dn_send.at[line + where, p],
            dn_recv.at[where, p],
            below,
        )

    def back_step(turn, _):
        step = line - 1 - turn % (line - 1)
        upward = (turn < line - 1) == (2 * z < line - 1)
        low, high = z - step, z + step

        def pass_on(where, chained, back, came, leaving):
            for p in range(halves):
                span = pl.ds(p * part_rows, part_rows)
                side_back(where, p).wait_recv()
                leaving[where, span, :] = (
                    own[where, span, :] + side_in[where, span, :].astype(jnp.float32)
                ).astype(jnp.bfloat16)

                @pl.when(chained)
                def _():
                    back(where, p).wait_recv()
                    leaving[where, span, :] = (
                        own[where, span, :]
                        + side_in[where, span, :].astype(jnp.float32)
                        + came[where, span, :].astype(jnp.float32)
                    ).astype(jnp.bfloat16)

                back(where, p).start()

        @pl.when(jnp.logical_and(upward, high < line))
        def _():
            pass_on(high, z > 0, up_back, up_in, up_out)

        @pl.when(jnp.logical_and(jnp.logical_not(upward), low >= 0))
        def _():
            pass_on(low, z < line - 1, dn_back, dn_in, dn_out)

        return 0

    lax.fori_loop(0, 2 * (line - 1), back_step, 0)
    for p in range(halves):
        side_back(z, p).wait_recv()
    base[...] += own[z] + side_in[z].astype(jnp.float32)

    @pl.when(z > 0)
    def _():
        for p in range(halves):
            up_back(z, p).wait_recv()
        base[...] += up_in[z].astype(jnp.float32)

    @pl.when(z < line - 1)
    def _():
        for p in range(halves):
            dn_back(z, p).wait_recv()
        base[...] += dn_in[z].astype(jnp.float32)

    out_ref[...] = base[...].astype(jnp.bfloat16)
    for j in range(1, sp_count):
        gate_move(j).wait_send()
    for i in range(2):
        core_copy(i).wait_send()
    hop.wait_send()

    def drain(where, _):
        for p in range(halves):
            send_side(where, p).wait_send()
            side_back(where, p).wait_send()

            @pl.when(jnp.logical_and(where <= z, z < line - 1))
            def _():
                send_up(where, p).wait_send()

            @pl.when(jnp.logical_and(where >= z, z > 0))
            def _():
                send_dn(where, p).wait_send()

            @pl.when(where > z)
            def _():
                up_back(where, p).wait_send()

            @pl.when(where < z)
            def _():
                dn_back(where, p).wait_send()

        return 0

    lax.fori_loop(0, line, drain, 0)


def tail_fused(
    attended,
    residual,
    norm_gain,
    expert_ids,
    route_weights,
    out_weight,
    expert_gate,
    expert_up,
    expert_down,
    shared_gate,
    shared_up,
    shared_down,
    sp_count,
):
    rows, width = residual.shape
    line = sp_count // 2
    table = (sp_count, 8, rows)
    vmem, hbm = pl.BlockSpec(memory_space=pltpu.VMEM), pl.BlockSpec(memory_space=pl.ANY)
    bf16, f32 = jnp.bfloat16, jnp.float32
    loaded = (
        out_weight,
        expert_gate[0],
        expert_up[0],
        expert_down[0],
        shared_gate,
        shared_up,
        shared_down,
    )
    dma = pltpu.SemaphoreType.DMA
    one = (rows, width)
    return pl.pallas_call(
        functools.partial(tail_kernel, sp_count),
        out_shape=jax.ShapeDtypeStruct(one, bf16),
        in_specs=[vmem] * 5 + [hbm] * 7,
        out_specs=vmem,
        scratch_shapes=[pltpu.VMEM(w.shape, bf16) for w in loaded]
        + [
            pltpu.VMEM(table, f32),
            pltpu.VMEM(table, f32),
            pltpu.VMEM((2,) + one, bf16),
            pltpu.VMEM((2,) + one, bf16),
            pltpu.VMEM((2,) + one, f32),
            pltpu.VMEM(one, bf16),
            pltpu.VMEM(one, bf16),
            pltpu.VMEM(one, f32),
            pltpu.VMEM((sp_count,) + one, bf16),
            pltpu.VMEM((line,) + one, bf16),
            pltpu.VMEM((line,) + one, bf16),
            pltpu.VMEM((line,) + one, f32),
            pltpu.VMEM((line,) + one, bf16),
            pltpu.VMEM((line,) + one, bf16),
            pltpu.VMEM((line,) + one, bf16),
            pltpu.VMEM((line,) + one, bf16),
            dma((7,)),
            dma((sp_count - 1,)),
            dma((sp_count - 1,)),
            dma((2, 2)),
            dma((2,)),
            dma((sp_count, 2)),
            dma((2 * line, 2)),
            dma((line, 2)),
            dma((2 * line, 2)),
            dma((line, 2)),
            dma((2 * line, 2)),
            dma((line, 2)),
        ],
        compiler_params=pltpu.CompilerParams(
            collective_id=1, has_side_effects=True, vmem_limit_bytes=60 * 2**20
        ),
    )(attended, residual, norm_gain[None, :], expert_ids.T, route_weights.T, *loaded)


def absorb_group(carried, query_group, shard_piece, sum_piece, score_scale):
    query_heads, query_sums, query_pos, last_pos = query_group
    key_piece, value_piece = shard_piece
    piece_rows = key_piece.shape[0]
    query_count, local_kv, group_size, head_size = query_heads.shape
    key_block = math.gcd(piece_rows, 1024)
    key_heads = key_piece.reshape(piece_rows, local_kv, head_size)
    value_heads = value_piece.reshape(piece_rows, local_kv, head_size)
    key_sums = sum_piece.reshape(piece_rows, local_kv, group_size).transpose(1, 2, 0)

    def update(block_start, held):
        row_max, row_sum, weighted = held
        key_part = lax.dynamic_slice_in_dim(key_heads, block_start, key_block, 0)
        value_part = lax.dynamic_slice_in_dim(value_heads, block_start, key_block, 0)
        sums_part = lax.dynamic_slice_in_dim(key_sums, block_start, key_block, 2)
        scores = (
            jnp.einsum("qhgd,khd->hgqk", query_heads, key_part, preferred_element_type=jnp.float32)
            * score_scale
        )
        scores = scores + (query_sums[:, :, :, None] - sums_part[:, :, None, :])
        key_pos = block_start + jnp.arange(key_block, dtype=jnp.int32)
        allowed = query_pos[:, None] >= key_pos[None, :]
        scores = jnp.where(allowed, scores, -jnp.inf)
        new_max = jnp.maximum(row_max, jnp.max(scores, axis=3))
        weights = jnp.exp(scores - new_max[:, :, :, None])
        factor = jnp.exp(row_max - new_max)
        row_sum = row_sum * factor + jnp.sum(weights, axis=3)
        products = jnp.einsum(
            "hgqk,khd->qhgd",
            weights.astype(jnp.bfloat16),
            value_part,
            preferred_element_type=jnp.float32,
        )
        weighted = weighted * factor.transpose(2, 0, 1)[:, :, :, None] + products
        return (new_max, row_sum, weighted)

    def one_block(block_index, held):
        block_start = block_index * key_block
        needed = block_start <= last_pos
        return lax.cond(needed, lambda inner: update(block_start, inner), lambda inner: inner, held)

    return lax.fori_loop(0, piece_rows // key_block, one_block, carried)


def finish(carried):
    row_max, row_sum, weighted = carried
    mixed = weighted / row_sum.transpose(2, 0, 1)[:, :, :, None]
    return mixed.reshape(mixed.shape[0], -1).astype(jnp.bfloat16)


def local(
    residual,
    queries,
    key_rows,
    value_rows,
    forget_sums,
    out_weight,
    norm_gain,
    expert_ids,
    route_weights,
    expert_gate,
    expert_up,
    expert_down,
    shared_gate,
    shared_up,
    shared_down,
):
    sp_count = lax.axis_size("sp")
    sp_index = lax.axis_index("sp")
    local_rows = queries.shape[0]
    local_kv = key_rows.shape[1] // HEAD_DIM
    group_size = HEADS // KV_HEADS
    score_scale = HEAD_DIM ** (-0.5)
    tp_count = lax.axis_size("tp")
    tokens_here = residual.shape[0]
    every_slot = 2 * tokens_here * TOPK >= tokens_here * expert_gate.shape[0] * sp_count
    if every_slot and expert_gate.shape[0] == 1 and sp_count % 2 == 0 and sp_count > 4 and tp_count == 4:
        attended = attend_fused(queries, key_rows, value_rows, forget_sums, sp_count)
        return tail_fused(
            attended,
            residual,
            norm_gain,
            expert_ids,
            route_weights,
            out_weight,
            expert_gate,
            expert_up,
            expert_down,
            shared_gate,
            shared_up,
            shared_down,
            sp_count,
        )
    own_first = sp_index * local_rows
    all_sums = lax.all_gather(forget_sums, "sp", axis=0, tiled=True)
    positions = own_first + jnp.arange(local_rows, dtype=jnp.int32)
    groups = [
        (
            queries.reshape(queries.shape[0], local_kv, group_size, HEAD_DIM),
            forget_sums.reshape(forget_sums.shape[0], local_kv, group_size).transpose(1, 2, 0),
            positions,
            positions[-1],
        )
    ]

    def initial(query_count):
        return (
            jnp.full((local_kv, group_size, query_count), -1e30, jnp.float32),
            jnp.zeros((local_kv, group_size, query_count), jnp.float32),
            jnp.zeros((query_count, local_kv, group_size, HEAD_DIM), jnp.float32),
        )

    def absorb(states, shard_piece):
        return tuple(
            (
                absorb_group(held, query_group, shard_piece, all_sums, score_scale)
                for held, query_group in zip(states, groups)
            )
        )

    start_states = tuple((initial(query_group[0].shape[0]) for query_group in groups))
    states = absorb(
        start_states,
        (
            lax.all_gather(key_rows, "sp", axis=0, tiled=True),
            lax.all_gather(value_rows, "sp", axis=0, tiled=True),
        ),
    )
    outputs = [finish(held) for held in states]
    attended = outputs[0]
    rows_out = local_rows // lax.axis_size("tp")
    branch = lax.psum_scatter(
        jnp.dot(attended, out_weight, preferred_element_type=jnp.float32).astype(jnp.bfloat16),
        "tp",
        scatter_dimension=0,
        tiled=True,
    ).astype(jnp.float32)
    stream = (residual.astype(jnp.float32) + branch).astype(jnp.bfloat16)
    wide = lax.optimization_barrier(stream).astype(jnp.float32)
    normed = (
        wide * lax.rsqrt(jnp.mean(wide * wide, axis=1, keepdims=True) + norm_eps) * norm_gain
    ).astype(jnp.bfloat16)
    width = normed.shape[1]
    experts_here = expert_gate.shape[0]
    total_experts = experts_here * sp_count
    capacity = 2 * rows_out * TOPK // total_experts
    flat_ids = expert_ids.reshape(-1)
    assigned = flat_ids.shape[0]
    onehot = (flat_ids[:, None] == jnp.arange(total_experts, dtype=jnp.int32)[None, :]).astype(
        jnp.int32
    )
    slot_rank = jnp.sum((jnp.cumsum(onehot, axis=0) - 1) * onehot, axis=1)
    target = flat_ids * capacity + slot_rank
    slot_count = total_experts * capacity
    source = (
        jnp.full((slot_count,), assigned, jnp.int32)
        .at[target]
        .set(jnp.arange(assigned, dtype=jnp.int32))
    )
    padded = jnp.concatenate([normed, jnp.zeros((1, width), jnp.bfloat16)], axis=0)
    outgoing = padded[source // TOPK].reshape(sp_count, experts_here, capacity, width)
    arrived = lax.all_to_all(outgoing, "sp", split_axis=0, concat_axis=0, tiled=True)
    gate_part = jnp.einsum(
        "necd,edf->necf", arrived, expert_gate, preferred_element_type=jnp.float32
    )
    up_part = jnp.einsum("necd,edf->necf", arrived, expert_up, preferred_element_type=jnp.float32)
    hidden = (jax.nn.silu(gate_part) * up_part).astype(jnp.bfloat16)
    processed = jnp.einsum(
        "necf,efd->necd", hidden, expert_down, preferred_element_type=jnp.float32
    ).astype(jnp.bfloat16)
    returned = lax.all_to_all(processed, "sp", split_axis=0, concat_axis=0, tiled=True)
    results = returned.reshape(slot_count, width)
    picked = results[target].reshape(rows_out, TOPK, width).astype(jnp.float32)
    gates = route_weights / jnp.sum(route_weights, axis=1, keepdims=True) * routed_scale
    routed = jnp.sum(gates[:, :, None] * picked, axis=1)
    shared_hidden = (
        jax.nn.silu(jnp.dot(normed, shared_gate, preferred_element_type=jnp.float32))
        * jnp.dot(normed, shared_up, preferred_element_type=jnp.float32)
    ).astype(jnp.bfloat16)
    shared_out = jnp.dot(shared_hidden, shared_down, preferred_element_type=jnp.float32)
    return (wide + shared_out + routed).astype(jnp.bfloat16)


def solution(mesh):
    in_specs = (
        P(("sp", "tp"), None),
        P("sp", "tp"),
        P("sp", "tp"),
        P("sp", "tp"),
        P("sp", "tp"),
        P("tp", None),
        P(),
        P(("sp", "tp"), None),
        P(("sp", "tp"), None),
        P("sp", None, None),
        P("sp", None, None),
        P("sp", None, None),
        P(),
        P(),
        P(),
    )
    out_specs = P(("sp", "tp"), None)
    return jax.shard_map(local, mesh=mesh, in_specs=in_specs, out_specs=out_specs, check_vma=False)
```

```python
import functools
import math

import jax
import jax.numpy as jnp
from jax import lax
from jax.experimental import pallas as pl
from jax.experimental.pallas import tpu as pltpu
from jax.sharding import PartitionSpec as P

HEADS = 16
KV_HEADS = 8
HEAD_DIM = 128
TOPK = 4


routed_scale = 2.5
norm_eps = 1e-06


MESH_ID = pl.DeviceIdType.MESH
LOG2E = math.log2(math.e)


def remote(src, dst, send_sem, recv_sem, target):
    return pltpu.make_async_remote_copy(
        src_ref=src,
        dst_ref=dst,
        send_sem=send_sem,
        recv_sem=recv_sem,
        device_id=target,
        device_id_type=MESH_ID,
    )


def greet(barrier, target):
    pl.semaphore_signal(barrier, inc=1, device_id=target, device_id_type=MESH_ID)


def attend_kernel(
    enter,
    sp_count,
    score_scale,
    q_ref,
    f_ref,
    k_hbm,
    v_hbm,
    out_ref,
    kbuf,
    vbuf,
    fbuf,
    qs,
    fqs,
    acc,
    top,
    den,
    load_sem,
    up_sem,
    side_sem,
    recv_sem,
):
    me, tp = lax.axis_index("sp"), lax.axis_index("tp")
    line = sp_count // 2
    z, y = me // 2, me % 2
    mate = (2 * z + 1 - y, tp)
    above = (jnp.minimum(me + 2, sp_count - 1), tp)
    below = (jnp.maximum(me - 2, 0), tp)
    bufs = (kbuf, vbuf, fbuf)
    loads = [
        pltpu.make_async_copy(src, buf.at[me], load_sem.at[i])
        for i, (src, buf) in enumerate(zip((k_hbm, v_hbm), bufs))
    ]
    for copy in loads:
        copy.start()
    fbuf[me] = jnp.zeros(fbuf.shape[1:], jnp.float32)
    fbuf[me, : f_ref.shape[0], :] = f_ref[...]
    rows, pair = q_ref.shape[0], qs.shape[1] // q_ref.shape[0]
    kv_heads = qs.shape[0]
    for h in range(kv_heads * pair):
        qs[h // pair, (h % pair) * rows : (h % pair + 1) * rows, :] = q_ref[
            :, h * HEAD_DIM : (h + 1) * HEAD_DIM
        ]
    square = (rows, rows)
    diagonal = lax.broadcasted_iota(jnp.int32, square, 0) == lax.broadcasted_iota(jnp.int32, square, 1)
    for h in range(kv_heads * pair):
        column = jnp.sum(jnp.where(diagonal, f_ref[h : h + 1, :], 0.0), axis=1, keepdims=True)
        fqs[h // pair, (h % pair) * rows : (h % pair + 1) * rows, :] = jnp.broadcast_to(
            column, (rows, HEAD_DIM)
        )
    for copy in loads:
        copy.wait()
    enter()

    def moves(block, step, sems, target):
        return [
            remote(buf.at[block], buf.at[block], sems.at[step, i], recv_sem.at[block, i], target)
            for i, buf in enumerate(bufs)
        ]

    def forward(step, arriving):
        block = 2 * (z - step) + y
        for i in (2, 0, 1):
            if arriving:
                moves(block, step, up_sem, below)[i].wait_recv()

            @pl.when(z < line - 1)
            def _():
                moves(block, step, up_sem, above)[i].start()

            @pl.when(jnp.logical_or(y == 0, step > 0))
            def _():
                moves(block, step, side_sem, mate)[i].start()

    def absorb(block, first):
        for g in range(kv_heads):
            lanes = slice(g * HEAD_DIM, (g + 1) * HEAD_DIM)
            keys, values = kbuf[block, :, lanes], vbuf[block, :, lanes]
            products = lax.dot_general(
                qs[g], keys, (((1,), (1,)), ((), ())), preferred_element_type=jnp.float32
            )
            parts = []
            for j in range(pair):
                h = g * pair + j
                drop = fqs[g, j * rows : (j + 1) * rows, :1] - fbuf[block, h : h + 1, :]
                part = products[j * rows : (j + 1) * rows] * (score_scale * LOG2E) + drop * LOG2E
                if first:
                    at_row = lax.broadcasted_iota(jnp.int32, part.shape, 0)
                    at_col = lax.broadcasted_iota(jnp.int32, part.shape, 1)
                    part = jnp.where(at_row >= at_col, part, -jnp.inf)
                parts.append(part)
            scores = jnp.concatenate(parts, axis=0)
            peak = jnp.max(scores, axis=1, keepdims=True)
            if first:
                weights = jnp.exp2(scores - peak)
                total = jnp.sum(weights, axis=1, keepdims=True)
            else:
                old = top[g][:, :1]
                peak = jnp.maximum(old, peak)
                factor = jnp.exp2(old - peak)
                weights = jnp.exp2(scores - peak)
                total = den[g][:, :1] * factor + jnp.sum(weights, axis=1, keepdims=True)
            mixed = jnp.dot(weights.astype(jnp.bfloat16), values, preferred_element_type=jnp.float32)
            acc[g] = mixed if first else acc[g] * factor + mixed
            top[g] = jnp.broadcast_to(peak, top.shape[1:])
            den[g] = jnp.broadcast_to(total, den.shape[1:])

    forward(0, False)
    absorb(me, True)

    def one_step(step, _):
        @pl.when(step <= z)
        def _():
            block = 2 * (z - step) + y
            forward(step, True)
            absorb(block, False)

        @pl.when(jnp.logical_and(step - 1 <= z, jnp.logical_or(y == 1, step > 1)))
        def _():
            block = 2 * (z - step + 1) + 1 - y
            for copy in moves(block, step - 1, side_sem, mate):
                copy.wait_recv()
            absorb(block, False)

        return 0

    lax.fori_loop(1, line + 1, one_step, 0)
    for g in range(kv_heads):
        done = (acc[g] / den[g]).astype(jnp.bfloat16)
        for j in range(pair):
            h = g * pair + j
            out_ref[:, h * HEAD_DIM : (h + 1) * HEAD_DIM] = done[j * rows : (j + 1) * rows]

    def drain(step, _):
        @pl.when(step <= z)
        def _():
            block = 2 * (z - step) + y

            @pl.when(z < line - 1)
            def _():
                for copy in moves(block, step, up_sem, above):
                    copy.wait_send()

            @pl.when(jnp.logical_or(y == 0, step > 0))
            def _():
                for copy in moves(block, step, side_sem, mate):
                    copy.wait_send()

        return 0

    lax.fori_loop(0, line, drain, 0)


def tail_kernel(
    weights,
    sp_count,
    att_ref,
    res_ref,
    gain_ref,
    ids_ref,
    score_ref,
    wo_hbm,
    eg_hbm,
    eu_hbm,
    ed_hbm,
    sg_hbm,
    su_hbm,
    sd_hbm,
    out_ref,
    wo,
    eg,
    eu,
    ed,
    sg,
    su,
    sd,
    gate_in,
    gate_buf,
    core_out,
    core_in,
    kept,
    x_out,
    x_in,
    base,
    tok,
    side_out,
    side_in,
    own,
    up_out,
    up_in,
    dn_out,
    dn_in,
    load_sem,
    gsend_sem,
    grecv_sem,
    pair_sem,
    hop_sem,
    tok_sem,
    side_send,
    side_recv,
    up_send,
    up_recv,
    dn_send,
    dn_recv,
):
    me, tp = lax.axis_index("sp"), lax.axis_index("tp")
    line = sp_count // 2
    z, y = me // 2, me % 2
    x, c = tp // 2, tp % 2
    mate = (2 * z + 1 - y, tp)
    above = (jnp.minimum(me + 2, sp_count - 1), tp)
    below = (jnp.maximum(me - 2, 0), tp)
    core_mate = (me, 2 * x + 1 - c)
    x_mate = (me, 2 * (1 - x) + c)
    rows = res_ref.shape[0]
    scores = score_ref[...]
    gates = scores / jnp.sum(scores, axis=0, keepdims=True) * routed_scale
    for e in range(sp_count):
        row = jnp.sum(jnp.where(ids_ref[...] == e, gates, 0.0), axis=0, keepdims=True)
        gate_in[e] = jnp.broadcast_to(row, gate_in.shape[1:])
    weights[0].wait()

    def gate_move(j):
        peer, source = lax.rem(me + j, sp_count), me
        return remote(
            gate_in.at[peer], gate_buf.at[source], gsend_sem.at[j - 1], grecv_sem.at[j - 1], (peer, tp)
        )

    def gate_arrival(j):
        source = lax.rem(me - j + sp_count, sp_count)
        return remote(
            gate_in.at[source], gate_buf.at[source], gsend_sem.at[j - 1], grecv_sem.at[j - 1], (source, tp)
        )

    for j in range(1, sp_count):
        gate_move(j).start()

    far, near = (1 - x) * 2, x * 2

    def core_copy(i):
        return remote(core_out.at[i], core_in.at[i], pair_sem.at[0, i], pair_sem.at[1, i], core_mate)

    hop = remote(x_out, x_in, hop_sem.at[0], hop_sem.at[1], x_mate)

    def project(block):
        return jnp.dot(
            att_ref[pl.ds(pl.multiple_of(block * rows, rows), rows), :],
            wo[...],
            preferred_element_type=jnp.float32,
        )

    def project_to(i, _):
        out_x = jnp.where(i == 0, far, near)
        core_out[i] = project(out_x + 1 - c).astype(jnp.bfloat16)
        core_copy(i).start()
        kept[i] = project(out_x + c)
        core_copy(i).wait_recv()
        kept[i] = kept[i] + core_in[i].astype(jnp.float32)

        @pl.when(i == 0)
        def _():
            x_out[...] = kept[0].astype(jnp.bfloat16)
            hop.start()

        return 0

    lax.fori_loop(0, 2, project_to, 0)
    branch = kept[1] + res_ref[...].astype(jnp.float32)
    hop.wait_recv()
    stream = (branch + x_in[...].astype(jnp.float32)).astype(jnp.bfloat16)
    wide = stream.astype(jnp.float32)
    scale = lax.rsqrt(jnp.mean(wide * wide, axis=1, keepdims=True) + norm_eps)
    tok[me] = (wide * scale * gain_ref[...]).astype(jnp.bfloat16)
    base[...] = wide

    halves = 2
    part_rows = rows // halves

    def piece(ref, i, p):
        return ref.at[i, pl.ds(p * part_rows, part_rows), :]

    def tok_move(block, p, sem, target):
        return remote(piece(tok, block, p), piece(tok, block, p), sem, tok_sem.at[block, p], target)

    def block_of(where):
        return 2 * where + y

    def send_up(where, p):
        return tok_move(block_of(where), p, up_send.at[where, p], above)

    def send_dn(where, p):
        return tok_move(block_of(where), p, dn_send.at[where, p], below)

    def send_side(where, p):
        return tok_move(block_of(where), p, side_send.at[where, p], mate)

    for p in range(halves):
        send_side(z, p).start()

        @pl.when(z < line - 1)
        def _():
            send_up(z, p).start()

        @pl.when(z > 0)
        def _():
            send_dn(z, p).start()

    for copy in weights[1:]:
        copy.wait()

    def gated(inputs, gate, up, down):
        first = jnp.dot(inputs, gate[...], preferred_element_type=jnp.float32)
        second = jnp.dot(inputs, up[...], preferred_element_type=jnp.float32)
        hidden = (first / (1.0 + jnp.exp(-first)) * second).astype(jnp.bfloat16)
        return jnp.dot(hidden, down[...], preferred_element_type=jnp.float32)

    base[...] += gated(tok[me], sg, su, sd)
    for j in range(1, sp_count):
        gate_arrival(j).wait_recv()
    gate_buf[me] = gate_in[me]

    def expert(block):
        row = gate_buf[block][:1, :]
        shape = (rows, row.shape[1])
        diagonal = lax.broadcasted_iota(jnp.int32, shape, 0) == lax.broadcasted_iota(jnp.int32, shape, 1)
        column = jnp.sum(jnp.where(diagonal, row, 0.0), axis=1, keepdims=True)
        result = gated(tok[block], eg, eu, ed).astype(jnp.bfloat16).astype(jnp.float32)
        return result * column

    def side_back(where, p):
        return remote(
            piece(side_out, where, p),
            piece(side_in, where, p),
            side_send.at[line + where, p],
            side_recv.at[where, p],
            mate,
        )

    def inside(where):
        return jnp.logical_and(where >= 0, where < line)

    def mates_block(where):
        for p in range(halves):
            tok_move(2 * where + 1 - y, p, side_send.at[where, p], mate).wait_recv()
        side_out[where] = expert(2 * where + 1 - y).astype(jnp.bfloat16)

    def own_part(step):
        def at(i, _):
            where = jnp.where(i == 0, z - step, z + step)

            @pl.when(inside(where))
            def _():
                own[where] = expert(block_of(where))

            return 0

        lax.fori_loop(0, 2, at, 0)

    def mates_part(step):
        def at(i, _):
            where = jnp.where(i == 0, z - step, z + step)

            @pl.when(jnp.logical_and(inside(where), jnp.logical_or(i == 0, step > 0)))
            def _():
                mates_block(where)

            return 0

        lax.fori_loop(0, 2, at, 0)

    own[z] = expert(me)

    def one_step(step, _):
        low, high = z - step, z + step
        for p in range(halves):

            @pl.when(low >= 0)
            def _():
                tok_move(block_of(low), p, up_send.at[low, p], below).wait_recv()
                send_side(low, p).start()

                @pl.when(z < line - 1)
                def _():
                    send_up(low, p).start()

            @pl.when(high < line)
            def _():
                tok_move(block_of(high), p, dn_send.at[high, p], above).wait_recv()
                send_side(high, p).start()

                @pl.when(z > 0)
                def _():
                    send_dn(high, p).start()

        @pl.when(step == line - 1)
        def _():
            for p in range(halves):
                side_back(z, p).start()

        own_part(step)
        mates_part(step - 1)
        return 0

    lax.fori_loop(1, line, one_step, 0)
    mates_part(line - 1)

    def cross(turn, _):
        step = line - 1 - turn
        for where in (z - step, z + step):

            @pl.when(inside(where))
            def _():
                for p in range(halves):
                    side_back(where, p).start()

        return 0

    lax.fori_loop(0, line - 1, cross, 0)

    def up_back(where, p):
        return remote(
            piece(up_out, where, p),
            piece(up_in, where, p),
            up_send.at[line + where, p],
            up_recv.at[where, p],
            above,
        )

    def dn_back(where, p):
        return remote(
            piece(dn_out, where, p),
            piece(dn_in, where, p),
            dn_send.at[line + where, p],
            dn_recv.at[where, p],
            below,
        )

    def back_step(turn, _):
        step = line - 1 - turn % (line - 1)
        upward = (turn < line - 1) == (2 * z < line - 1)
        low, high = z - step, z + step

        def pass_on(where, chained, back, came, leaving):
            for p in range(halves):
                span = pl.ds(p * part_rows, part_rows)
                side_back(where, p).wait_recv()
                leaving[where, span, :] = (
                    own[where, span, :] + side_in[where, span, :].astype(jnp.float32)
                ).astype(jnp.bfloat16)

                @pl.when(chained)
                def _():
                    back(where, p).wait_recv()
                    leaving[where, span, :] = (
                        own[where, span, :]
                        + side_in[where, span, :].astype(jnp.float32)
                        + came[where, span, :].astype(jnp.float32)
                    ).astype(jnp.bfloat16)

                back(where, p).start()

        @pl.when(jnp.logical_and(upward, high < line))
        def _():
            pass_on(high, z > 0, up_back, up_in, up_out)

        @pl.when(jnp.logical_and(jnp.logical_not(upward), low >= 0))
        def _():
            pass_on(low, z < line - 1, dn_back, dn_in, dn_out)

        return 0

    lax.fori_loop(0, 2 * (line - 1), back_step, 0)
    for p in range(halves):
        side_back(z, p).wait_recv()
    base[...] += own[z] + side_in[z].astype(jnp.float32)

    @pl.when(z > 0)
    def _():
        for p in range(halves):
            up_back(z, p).wait_recv()
        base[...] += up_in[z].astype(jnp.float32)

    @pl.when(z < line - 1)
    def _():
        for p in range(halves):
            dn_back(z, p).wait_recv()
        base[...] += dn_in[z].astype(jnp.float32)

    out_ref[...] = base[...].astype(jnp.bfloat16)
    for j in range(1, sp_count):
        gate_move(j).wait_send()
    for i in range(2):
        core_copy(i).wait_send()
    hop.wait_send()

    def drain(where, _):
        for p in range(halves):
            send_side(where, p).wait_send()
            side_back(where, p).wait_send()

            @pl.when(jnp.logical_and(where <= z, z < line - 1))
            def _():
                send_up(where, p).wait_send()

            @pl.when(jnp.logical_and(where >= z, z > 0))
            def _():
                send_dn(where, p).wait_send()

            @pl.when(where > z)
            def _():
                up_back(where, p).wait_send()

            @pl.when(where < z)
            def _():
                dn_back(where, p).wait_send()

        return 0

    lax.fori_loop(0, line, drain, 0)


def layer_kernel(sp_count, score_scale, q_ref, f_ref, k_hbm, v_hbm, res_ref, gain_ref, ids_ref, score_ref, *rest):
    sources, out_ref, rest = rest[:7], rest[7], rest[8:]
    att_ref, attend_scratch, tail_scratch = rest[0], rest[1:13], rest[13:]
    load_sem = tail_scratch[23]
    me, tp = lax.axis_index("sp"), lax.axis_index("tp")
    x, c = tp // 2, tp % 2
    held = tail_scratch[:7]
    weights = [
        pltpu.make_async_copy(sources[i], held[i], load_sem.at[i]) for i in (0, 4, 5, 6, 1, 2, 3)
    ]
    barrier = pltpu.get_barrier_semaphore()
    greet(barrier, (me, 2 * x + 1 - c))
    greet(barrier, (me, 2 * (1 - x) + c))
    for j in range(1, sp_count):
        greet(barrier, (lax.rem(me + j, sp_count), tp))

    def enter():
        pl.semaphore_wait(barrier, sp_count + 1)
        for copy in weights:
            copy.start()

    attend_kernel(enter, sp_count, score_scale, q_ref, f_ref, k_hbm, v_hbm, att_ref, *attend_scratch)
    tail_kernel(
        weights, sp_count, att_ref, res_ref, gain_ref, ids_ref, score_ref, *sources, out_ref, *tail_scratch
    )


def layer_fused(
    residual,
    queries,
    key_rows,
    value_rows,
    forget_sums,
    norm_gain,
    expert_ids,
    route_weights,
    out_weight,
    expert_gate,
    expert_up,
    expert_down,
    shared_gate,
    shared_up,
    shared_down,
    sp_count,
):
    query_rows, heads = queries.shape[0], forget_sums.shape[1]
    kv_heads = key_rows.shape[1] // HEAD_DIM
    stacked = (kv_heads, heads // kv_heads * query_rows, HEAD_DIM)
    rows, width = residual.shape
    line = sp_count // 2
    table = (sp_count, 8, rows)
    vmem, hbm = pl.BlockSpec(memory_space=pltpu.VMEM), pl.BlockSpec(memory_space=pl.ANY)
    bf16, f32 = jnp.bfloat16, jnp.float32
    loaded = (
        out_weight,
        expert_gate[0],
        expert_up[0],
        expert_down[0],
        shared_gate,
        shared_up,
        shared_down,
    )
    dma = pltpu.SemaphoreType.DMA
    one = (rows, width)
    return pl.pallas_call(
        functools.partial(layer_kernel, sp_count, HEAD_DIM ** (-0.5)),
        out_shape=jax.ShapeDtypeStruct(one, bf16),
        in_specs=[vmem, vmem, hbm, hbm] + [vmem] * 4 + [hbm] * 7,
        out_specs=vmem,
        scratch_shapes=[
            pltpu.VMEM(queries.shape, bf16),
            pltpu.VMEM((sp_count,) + key_rows.shape, bf16),
            pltpu.VMEM((sp_count,) + value_rows.shape, bf16),
            pltpu.VMEM((sp_count, -(-heads // 8) * 8, query_rows), f32),
            pltpu.VMEM(stacked, bf16),
            pltpu.VMEM(stacked, f32),
            pltpu.VMEM(stacked, f32),
            pltpu.VMEM(stacked, f32),
            pltpu.VMEM(stacked, f32),
            dma((2,)),
            dma((line, 3)),
            dma((line, 3)),
            dma((sp_count, 3)),
        ]
        + [pltpu.VMEM(w.shape, bf16) for w in loaded]
        + [
            pltpu.VMEM(table, f32),
            pltpu.VMEM(table, f32),
            pltpu.VMEM((2,) + one, bf16),
            pltpu.VMEM((2,) + one, bf16),
            pltpu.VMEM((2,) + one, f32),
            pltpu.VMEM(one, bf16),
            pltpu.VMEM(one, bf16),
            pltpu.VMEM(one, f32),
            pltpu.VMEM((sp_count,) + one, bf16),
            pltpu.VMEM((line,) + one, bf16),
            pltpu.VMEM((line,) + one, bf16),
            pltpu.VMEM((line,) + one, f32),
            pltpu.VMEM((line,) + one, bf16),
            pltpu.VMEM((line,) + one, bf16),
            pltpu.VMEM((line,) + one, bf16),
            pltpu.VMEM((line,) + one, bf16),
            dma((7,)),
            dma((sp_count - 1,)),
            dma((sp_count - 1,)),
            dma((2, 2)),
            dma((2,)),
            dma((sp_count, 2)),
            dma((2 * line, 2)),
            dma((line, 2)),
            dma((2 * line, 2)),
            dma((line, 2)),
            dma((2 * line, 2)),
            dma((line, 2)),
        ],
        compiler_params=pltpu.CompilerParams(
            collective_id=0, has_side_effects=True, vmem_limit_bytes=60 * 2**20
        ),
    )(
        queries,
        forget_sums.T,
        key_rows,
        value_rows,
        residual,
        norm_gain[None, :],
        expert_ids.T,
        route_weights.T,
        *loaded,
    )


def absorb_group(carried, query_group, shard_piece, sum_piece, score_scale):
    query_heads, query_sums, query_pos, last_pos = query_group
    key_piece, value_piece = shard_piece
    piece_rows = key_piece.shape[0]
    query_count, local_kv, group_size, head_size = query_heads.shape
    key_block = math.gcd(piece_rows, 1024)
    key_heads = key_piece.reshape(piece_rows, local_kv, head_size)
    value_heads = value_piece.reshape(piece_rows, local_kv, head_size)
    key_sums = sum_piece.reshape(piece_rows, local_kv, group_size).transpose(1, 2, 0)

    def update(block_start, held):
        row_max, row_sum, weighted = held
        key_part = lax.dynamic_slice_in_dim(key_heads, block_start, key_block, 0)
        value_part = lax.dynamic_slice_in_dim(value_heads, block_start, key_block, 0)
        sums_part = lax.dynamic_slice_in_dim(key_sums, block_start, key_block, 2)
        scores = (
            jnp.einsum("qhgd,khd->hgqk", query_heads, key_part, preferred_element_type=jnp.float32)
            * score_scale
        )
        scores = scores + (query_sums[:, :, :, None] - sums_part[:, :, None, :])
        key_pos = block_start + jnp.arange(key_block, dtype=jnp.int32)
        allowed = query_pos[:, None] >= key_pos[None, :]
        scores = jnp.where(allowed, scores, -jnp.inf)
        new_max = jnp.maximum(row_max, jnp.max(scores, axis=3))
        weights = jnp.exp(scores - new_max[:, :, :, None])
        factor = jnp.exp(row_max - new_max)
        row_sum = row_sum * factor + jnp.sum(weights, axis=3)
        products = jnp.einsum(
            "hgqk,khd->qhgd",
            weights.astype(jnp.bfloat16),
            value_part,
            preferred_element_type=jnp.float32,
        )
        weighted = weighted * factor.transpose(2, 0, 1)[:, :, :, None] + products
        return (new_max, row_sum, weighted)

    def one_block(block_index, held):
        block_start = block_index * key_block
        needed = block_start <= last_pos
        return lax.cond(needed, lambda inner: update(block_start, inner), lambda inner: inner, held)

    return lax.fori_loop(0, piece_rows // key_block, one_block, carried)


def finish(carried):
    row_max, row_sum, weighted = carried
    mixed = weighted / row_sum.transpose(2, 0, 1)[:, :, :, None]
    return mixed.reshape(mixed.shape[0], -1).astype(jnp.bfloat16)


def local(
    residual,
    queries,
    key_rows,
    value_rows,
    forget_sums,
    out_weight,
    norm_gain,
    expert_ids,
    route_weights,
    expert_gate,
    expert_up,
    expert_down,
    shared_gate,
    shared_up,
    shared_down,
):
    sp_count = lax.axis_size("sp")
    sp_index = lax.axis_index("sp")
    local_rows = queries.shape[0]
    local_kv = key_rows.shape[1] // HEAD_DIM
    group_size = HEADS // KV_HEADS
    score_scale = HEAD_DIM ** (-0.5)
    tp_count = lax.axis_size("tp")
    tokens_here = residual.shape[0]
    every_slot = 2 * tokens_here * TOPK >= tokens_here * expert_gate.shape[0] * sp_count
    if every_slot and expert_gate.shape[0] == 1 and sp_count % 2 == 0 and sp_count > 4 and tp_count == 4:
        return layer_fused(
            residual,
            queries,
            key_rows,
            value_rows,
            forget_sums,
            norm_gain,
            expert_ids,
            route_weights,
            out_weight,
            expert_gate,
            expert_up,
            expert_down,
            shared_gate,
            shared_up,
            shared_down,
            sp_count,
        )
    own_first = sp_index * local_rows
    all_sums = lax.all_gather(forget_sums, "sp", axis=0, tiled=True)
    positions = own_first + jnp.arange(local_rows, dtype=jnp.int32)
    groups = [
        (
            queries.reshape(queries.shape[0], local_kv, group_size, HEAD_DIM),
            forget_sums.reshape(forget_sums.shape[0], local_kv, group_size).transpose(1, 2, 0),
            positions,
            positions[-1],
        )
    ]

    def initial(query_count):
        return (
            jnp.full((local_kv, group_size, query_count), -1e30, jnp.float32),
            jnp.zeros((local_kv, group_size, query_count), jnp.float32),
            jnp.zeros((query_count, local_kv, group_size, HEAD_DIM), jnp.float32),
        )

    def absorb(states, shard_piece):
        return tuple(
            (
                absorb_group(held, query_group, shard_piece, all_sums, score_scale)
                for held, query_group in zip(states, groups)
            )
        )

    start_states = tuple((initial(query_group[0].shape[0]) for query_group in groups))
    states = absorb(
        start_states,
        (
            lax.all_gather(key_rows, "sp", axis=0, tiled=True),
            lax.all_gather(value_rows, "sp", axis=0, tiled=True),
        ),
    )
    outputs = [finish(held) for held in states]
    attended = outputs[0]
    rows_out = local_rows // lax.axis_size("tp")
    branch = lax.psum_scatter(
        jnp.dot(attended, out_weight, preferred_element_type=jnp.float32).astype(jnp.bfloat16),
        "tp",
        scatter_dimension=0,
        tiled=True,
    ).astype(jnp.float32)
    stream = (residual.astype(jnp.float32) + branch).astype(jnp.bfloat16)
    wide = lax.optimization_barrier(stream).astype(jnp.float32)
    normed = (
        wide * lax.rsqrt(jnp.mean(wide * wide, axis=1, keepdims=True) + norm_eps) * norm_gain
    ).astype(jnp.bfloat16)
    width = normed.shape[1]
    experts_here = expert_gate.shape[0]
    total_experts = experts_here * sp_count
    capacity = 2 * rows_out * TOPK // total_experts
    flat_ids = expert_ids.reshape(-1)
    assigned = flat_ids.shape[0]
    onehot = (flat_ids[:, None] == jnp.arange(total_experts, dtype=jnp.int32)[None, :]).astype(
        jnp.int32
    )
    slot_rank = jnp.sum((jnp.cumsum(onehot, axis=0) - 1) * onehot, axis=1)
    target = flat_ids * capacity + slot_rank
    slot_count = total_experts * capacity
    source = (
        jnp.full((slot_count,), assigned, jnp.int32)
        .at[target]
        .set(jnp.arange(assigned, dtype=jnp.int32))
    )
    padded = jnp.concatenate([normed, jnp.zeros((1, width), jnp.bfloat16)], axis=0)
    outgoing = padded[source // TOPK].reshape(sp_count, experts_here, capacity, width)
    arrived = lax.all_to_all(outgoing, "sp", split_axis=0, concat_axis=0, tiled=True)
    gate_part = jnp.einsum(
        "necd,edf->necf", arrived, expert_gate, preferred_element_type=jnp.float32
    )
    up_part = jnp.einsum("necd,edf->necf", arrived, expert_up, preferred_element_type=jnp.float32)
    hidden = (jax.nn.silu(gate_part) * up_part).astype(jnp.bfloat16)
    processed = jnp.einsum(
        "necf,efd->necd", hidden, expert_down, preferred_element_type=jnp.float32
    ).astype(jnp.bfloat16)
    returned = lax.all_to_all(processed, "sp", split_axis=0, concat_axis=0, tiled=True)
    results = returned.reshape(slot_count, width)
    picked = results[target].reshape(rows_out, TOPK, width).astype(jnp.float32)
    gates = route_weights / jnp.sum(route_weights, axis=1, keepdims=True) * routed_scale
    routed = jnp.sum(gates[:, :, None] * picked, axis=1)
    shared_hidden = (
        jax.nn.silu(jnp.dot(normed, shared_gate, preferred_element_type=jnp.float32))
        * jnp.dot(normed, shared_up, preferred_element_type=jnp.float32)
    ).astype(jnp.bfloat16)
    shared_out = jnp.dot(shared_hidden, shared_down, preferred_element_type=jnp.float32)
    return (wide + shared_out + routed).astype(jnp.bfloat16)


def solution(mesh):
    in_specs = (
        P(("sp", "tp"), None),
        P("sp", "tp"),
        P("sp", "tp"),
        P("sp", "tp"),
        P("sp", "tp"),
        P("tp", None),
        P(),
        P(("sp", "tp"), None),
        P(("sp", "tp"), None),
        P("sp", None, None),
        P("sp", None, None),
        P("sp", None, None),
        P(),
        P(),
        P(),
    )
    out_specs = P(("sp", "tp"), None)
    return jax.shard_map(local, mesh=mesh, in_specs=in_specs, out_specs=out_specs, check_vma=False)
```
